256 devices in a mesh: ep: 64 (over z, y, core), tp: 4 (over x).
Axes of the slice: x: 4, y: 4, z: 8, core: 2. Of those that a mesh axis runs over, the one named last changes fastest.
Arguments:
- queries: bfloat16 [8192, 512], P('ep', 'tp'), may hold values from -8 to 8
- key_cache: bfloat16 [4, 64, 8192], P('tp', None, 'ep'), may hold values from -4.5 to 4.5
- value_cache: bfloat16 [4, 64, 8192], P('tp', None, 'ep'), may hold values from -6 to 6
- cum_gate: float32 [4, 8192], P('tp'), may hold values from -2048 to 0, as said below
- out_weight: bfloat16 [512, 2048], replicated, may hold values from -1 to 1
- routed_input: bfloat16 [16384, 2048], P('ep'), may hold values from -6 to 6
- norm_gain: bfloat16 [2048], replicated, may hold values from 0.099609375 to 1.8984375
- routes: int32 [16384, 2], P('ep'), may hold values from 0 to 63, all different within a row; in each aligned block of 64 rows (0 to 63, 64 to 127, ...) at most 3 rows name the same one
- route_weight: float32 [16384, 2], P('ep'), may hold values from 0.2 to 1
- expert_gate: bfloat16 [64, 2048, 1024], P('ep', None, 'tp'), may hold values from -0.125 to 0.125
- expert_up: bfloat16 [64, 2048, 1024], P('ep', None, 'tp'), may hold values from -0.125 to 0.125
- expert_down: bfloat16 [64, 1024, 2048], P('ep', 'tp'), may hold values from -0.1875 to 0.1875
Outputs:
- mixed_out: bfloat16 [8192, 2048], P(('ep', 'tp'))
- expert_out: bfloat16 [16384, 2048], P(('ep', 'tp'))
The draws below stay inside these ranges and needn't reach their ends.
Inputs may be any that keep to these rules, and one draw needn't show every extreme that they name: `cum_gate`: Non-increasing along positions in every head. `routes`: each row names 2 different experts. In each aligned block of 64 rows (the rows of one device) no expert is named by more than 3 rows, a bound that some block reaches.
All inputs are finite; a program needn't handle non-finite values.
Results may differ from the reference program's by a relative error of at most 0.012.
Values may be sent and summed in bfloat16 or wider, within the bound.
No kernel may reach another device: no remote copies, remote signals or barrier semaphores. Data moves between devices by JAX's collectives and lax.ppermute only.
A program may use at most 64 MiB of HBM per device.

```python
import math
import jax
import jax.numpy as jnp
import numpy as np
from jax import lax

D = 2048
HEADS = 8
HEAD = 64
KV_HEADS = 4
FFE = 1024
TOPK = 2
SEQ_ROWS = 128
TOK_DEV = 64
FIRST_TOKENS = 8192
ROUTED_TOKENS = 16384
EXPERTS = 64
CAP = 3
N_TP = 4


def draw_queries(key, part):
    base_key = jax.random.fold_in(key, 11)
    values = jnp.clip(jax.random.normal(base_key, (FIRST_TOKENS, HEADS * HEAD), jnp.float32), -4.0, 4.0)
    return values.astype(jnp.bfloat16)


def draw_key_cache(key, part):
    base_key = jax.random.fold_in(key, 13)
    values = jnp.clip(jax.random.normal(base_key, (KV_HEADS, HEAD, FIRST_TOKENS), jnp.float32), -4.0, 4.0)
    return values.astype(jnp.bfloat16)


def draw_cum_gate(key, part):
    ordering_random_key, gradual_random_key, quick_random_key, block_random_key, coarse_random_key, spike_random_key, loss_random_key = jax.random.split(jax.random.fold_in(key, 17), 7)
    ranks = jax.random.permutation(ordering_random_key, KV_HEADS)
    gradual_decay = ranks < KV_HEADS // 2
    rough = jax.random.uniform(coarse_random_key, (KV_HEADS, FIRST_TOKENS), jnp.float32, 0.2, 1.8)
    slow_rate = jax.random.uniform(gradual_random_key, (KV_HEADS,), jnp.float32, 0.1, 0.4) / FIRST_TOKENS
    fast_rate = 1.0 / jax.random.uniform(quick_random_key, (KV_HEADS,), jnp.float32, 30.0, 100.0)
    rate = jnp.where(gradual_decay, slow_rate, fast_rate)
    factor = jnp.exp(jax.random.uniform(block_random_key, (FIRST_TOKENS // SEQ_ROWS,), jnp.float32, -0.7, 0.7))
    per_position = jnp.repeat(factor, SEQ_ROWS)
    update_steps = -rate[:, None] * per_position[None, :] * rough
    marked_positions = jax.random.randint(spike_random_key, (2,), 0, FIRST_TOKENS)
    loss_values = jnp.log(jax.random.uniform(loss_random_key, (2,), jnp.float32, 0.5, 0.8))
    sudden_spike = jnp.zeros((FIRST_TOKENS,), jnp.float32).at[marked_positions].add(loss_values)
    update_steps = update_steps + jnp.where(gradual_decay[:, None], sudden_spike[None, :], 0.0)
    return jnp.cumsum(update_steps, axis=1)


def block_scale(stream_key, shape, cuts, low, largest):
    gain, own = 1.0, jax.random.fold_in(stream_key, 6)
    for dim, shards_of in cuts:
        draws = jnp.exp(jax.random.uniform(jax.random.fold_in(own, dim), (shards_of,), jnp.float32, low / len(cuts), largest / len(cuts)))
        gain = gain * jnp.repeat(draws, shape[dim] // shards_of).reshape([-1 if axis == dim else 1 for axis in range(len(shape))])
    return gain


def routed_block(stream_key, own, number, rows, count, top, bound, lean):
    order = jax.random.permutation(stream_key, count)
    packed, usual = load_shares(count, rows * top, bound, lean, True), load_shares(count, rows * top, bound, lean, False)
    places = jnp.arange(count)

    def named(sizes, turn):
        used = int((sizes > 0).sum())
        fixed = max(1, used // 4)
        passed = fixed + (places - fixed + turn * (used - fixed)) % max(1, count - fixed)
        return jnp.zeros((count,), jnp.int32).at[order[jnp.where(places < fixed, places, passed)]].set(jnp.asarray(sizes, jnp.int32))

    sizes = jnp.where(number % 4 == 0, named(packed, number // 4), named(usual, number - number // 4 - 1))
    mixed = jax.random.permutation(jax.random.fold_in(own, 3), count)
    donor, taker = mixed[0:count // 2 * 2:2], mixed[1:count // 2 * 2:2]
    margin = jnp.minimum(sizes[donor] - 1, bound - sizes[taker]) // 2
    margin = jnp.where((donor == order[0]) | (taker == order[0]) | (sizes[taker] == 0), 0, jnp.maximum(margin, 0))
    passed = jax.random.randint(jax.random.fold_in(own, 4), (count // 2,), 0, 1 << 20) % (margin + 1)
    sizes = sizes.at[donor].add(-passed).at[taker].add(passed)
    members = jnp.searchsorted(jnp.cumsum(sizes), jnp.arange(rows * top), side="right").astype(jnp.int32)
    table = members.reshape(top, rows).T
    table = table[jax.random.permutation(jax.random.fold_in(own, 1), rows)]
    turn = jax.random.randint(jax.random.fold_in(own, 2), (rows, 1), 0, top)
    return jnp.take_along_axis(table, (jnp.arange(top)[None, :] + turn) % top, axis=1)


def load_shares(amount, total, bound, slope, full):
    loads = [(1 << 20) // math.isqrt(rank ** slope) + 1 for rank in range(1, amount + 1)]
    largest = bound if full else min(bound, max(-(-total // amount), total * loads[0] // sum(loads)))
    least = 1 if total - largest >= amount - 1 else 0
    counts, spare = [largest] + [least] * (amount - 1), total - largest - least * (amount - 1)
    while spare > 0:
        movable = [i for i in range(1, amount) if counts[i] < largest] or [i for i in range(1, amount) if counts[i] < bound]
        whole, budget = sum([loads[i] for i in movable]), spare
        for i in movable:
            addition = min(bound - counts[i], max(1, budget * loads[i] // whole), spare)
            counts[i] = counts[i] + addition
            spare = spare - addition
    return np.array(counts)


def centred(key, dims, spread, bound, pieces=(), kind=jnp.bfloat16):
    result = jax.random.normal(key, dims, jnp.float32) * spread
    if len(pieces) > 0:
        result = block_scale(key, dims, pieces, -0.22, 0.18) * result
    return jnp.clip(result, min=-bound, max=bound).astype(kind)


def setup_inputs(seed: int = 0) -> dict:
    keys = jax.random.split(jax.random.key(seed), 13)
    queries = draw_queries(jax.random.fold_in(keys[12], 71), 0)
    key_cache = draw_key_cache(jax.random.fold_in(keys[12], 71), 0)
    value_cache = centred(keys[2], (KV_HEADS, HEAD, FIRST_TOKENS), 1.0, 6.0, ((0, 4), (2, 64)))
    cum_gate = draw_cum_gate(jax.random.fold_in(keys[12], 71), 0)
    out_weight = centred(keys[4], (HEADS * HEAD, D), (HEADS * HEAD // 16) ** -0.5, 1.0)
    routed_input = centred(keys[5], (ROUTED_TOKENS, D), 1.0, 6.0, ((0, 64),))
    norm_gain = jnp.clip(1.0 + 0.18 * jax.random.normal(keys[6], (D,), jnp.float32), 0.099609375, 1.8984375).astype(jnp.bfloat16)
    routes_keys = jax.random.split(jax.random.fold_in(keys[7], 1), ROUTED_TOKENS // TOK_DEV)
    routes_turns = jax.random.permutation(jax.random.fold_in(keys[7], 3), ROUTED_TOKENS // TOK_DEV)
    routes = jax.vmap(lambda own, number: routed_block(jax.random.fold_in(keys[7], 2), own, number, TOK_DEV, EXPERTS, TOPK, CAP, 1))(routes_keys, routes_turns).reshape((ROUTED_TOKENS, TOPK))
    route_weight = jnp.clip(0.2 + 0.8 * jax.random.uniform(keys[8], (ROUTED_TOKENS, TOPK), jnp.float32) ** block_scale(keys[8], (ROUTED_TOKENS, TOPK), ((0, 64),), -0.2, 0.2), 0.2, 1.0)
    expert_gate = centred(keys[9], (EXPERTS, D, FFE), D ** -0.5, 0.125, ((0, 64), (2, 4)))
    expert_up = centred(keys[10], (EXPERTS, D, FFE), D ** -0.5, 0.125, ((0, 64), (2, 4)))
    expert_down = centred(keys[11], (EXPERTS, FFE, D), FFE ** -0.5, 0.1875, ((0, 64), (1, 4)))
    return dict(queries=queries, key_cache=key_cache, value_cache=value_cache, cum_gate=cum_gate, out_weight=out_weight, routed_input=routed_input, norm_gain=norm_gain, routes=routes, route_weight=route_weight, expert_gate=expert_gate, expert_up=expert_up, expert_down=expert_down)


def attend_block(query_block, keys_head, values_head, gate_head, block_start):
    rows_here = query_block.shape[0]
    scores = jnp.einsum('tgd,ds->tgs', query_block, keys_head) * HEAD ** (-0.5)
    query_pos = block_start + jnp.arange(rows_here, dtype=jnp.int32)
    gate_query = lax.dynamic_slice_in_dim(gate_head, block_start, rows_here, 0)
    scores = scores + gate_query[:, None, None] - gate_head[None, None, :]
    key_pos = jnp.arange(FIRST_TOKENS, dtype=jnp.int32)
    allowed = key_pos[None, :] <= query_pos[:, None]
    scores = jnp.where(allowed[:, None, :], scores, -jnp.inf)
    highest = lax.optimization_barrier(jnp.max(scores, axis=-1, keepdims=True))
    weights = jnp.exp(scores - highest)
    total = lax.optimization_barrier(jnp.sum(weights, axis=-1))
    rounded = lax.optimization_barrier(weights.astype(jnp.bfloat16)).astype(jnp.float32)
    summed = jnp.einsum('tgs,ds->tgd', rounded, values_head)
    return (summed / total[..., None]).astype(jnp.bfloat16)

def reference(queries, key_cache, value_cache, cum_gate, out_weight, routed_input, norm_gain, routes, route_weight, expert_gate, expert_up, expert_down):
    group = HEADS // KV_HEADS
    nblocks = FIRST_TOKENS // SEQ_ROWS
    query_all = queries.astype(jnp.float32).reshape(nblocks, SEQ_ROWS, KV_HEADS, group, HEAD)
    keys_all = key_cache.astype(jnp.float32)
    values_all = value_cache.astype(jnp.float32)

    def one_pair(index):
        block = index // KV_HEADS
        head = index % KV_HEADS
        query_block = query_all[block, :, head]
        start = (block * SEQ_ROWS).astype(jnp.int32)
        return attend_block(query_block, keys_all[head], values_all[head], cum_gate[head], start)
    attended = lax.map(one_pair, jnp.arange(nblocks * KV_HEADS, dtype=jnp.int32))
    attended = attended.reshape(nblocks, KV_HEADS, SEQ_ROWS, group, HEAD).transpose(0, 2, 1, 3, 4).reshape(FIRST_TOKENS, HEADS * HEAD)
    mixed_out = jnp.dot(attended, out_weight, preferred_element_type=jnp.float32).astype(jnp.bfloat16)
    source = routed_input.astype(jnp.float32)
    scale = lax.rsqrt(lax.optimization_barrier(jnp.mean(source * source, axis=-1, keepdims=True)) + 1e-06)
    normed = (source * scale * norm_gain.astype(jnp.float32)).astype(jnp.bfloat16)
    nparts = ROUTED_TOKENS // TOK_DEV
    slots_all = EXPERTS * CAP
    pairs = routes.reshape(nparts, TOK_DEV * TOPK)
    same = (pairs[:, :, None] == jnp.arange(EXPERTS, dtype=jnp.int32)[None, None, :]).astype(jnp.int32)
    earlier = jnp.cumsum(same, axis=1) - same
    rank = lax.optimization_barrier(jnp.sum(earlier * same, axis=2))
    slot = pairs * CAP + rank
    chooser = (slot[:, :, None] == jnp.arange(slots_all, dtype=jnp.int32)[None, None, :]).astype(jnp.float32)
    chooser = chooser.reshape(nparts, TOK_DEV, TOPK, slots_all)
    normed_blocks = normed.astype(jnp.float32).reshape(nparts, TOK_DEV, D)
    width_part = FFE // N_TP

    def one_expert(expert):
        picks = lax.dynamic_slice_in_dim(chooser, expert * CAP, CAP, 3)
        gathered = jnp.einsum('btkc,btd->bcd', picks, normed_blocks).astype(jnp.bfloat16).reshape(nparts * CAP, D)
        gate = jnp.dot(gathered, expert_gate[expert], preferred_element_type=jnp.float32)
        upper = jnp.dot(gathered, expert_up[expert], preferred_element_type=jnp.float32)
        hidden = (jax.nn.silu(gate) * upper).astype(jnp.bfloat16)
        hidden_parts = hidden.astype(jnp.float32).reshape(nparts * CAP, N_TP, width_part)
        down_parts = expert_down[expert].astype(jnp.float32).reshape(N_TP, width_part, D)
        partial_value = jnp.einsum('rqf,qfd->qrd', hidden_parts, down_parts)
        partial_value = lax.optimization_barrier(partial_value.astype(jnp.bfloat16)).astype(jnp.float32)
        return lax.optimization_barrier(jnp.sum(partial_value, axis=0)).astype(jnp.bfloat16).reshape(nparts, CAP, D)
    results = lax.map(one_expert, jnp.arange(EXPERTS, dtype=jnp.int32))
    rank_blocks = rank.reshape(nparts, TOK_DEV, TOPK)
    expert_blocks = routes.reshape(nparts, TOK_DEV, TOPK)
    block_ids = jnp.arange(nparts, dtype=jnp.int32)[:, None, None]
    picked = results[expert_blocks, block_ids, rank_blocks].astype(jnp.float32)
    mixed_weights = route_weight.reshape(nparts, TOK_DEV, TOPK)[..., None] * picked
    expert_out = lax.optimization_barrier(jnp.sum(mixed_weights, axis=2)).reshape(ROUTED_TOKENS, D).astype(jnp.bfloat16)
    return (mixed_out, expert_out)
```

```python
import jax
import jax.numpy as jnp
from jax import lax
from jax.experimental import pallas as pl
from jax.experimental.pallas import tpu as pltpu
from jax.sharding import PartitionSpec as P


Z, Y, C = 8, 4, 2
TOK = 64
CAP = 3
EXPERTS = 64
SLOTS = EXPERTS * CAP
D = 2048
SUB = 16
TOP = 96
F32 = jnp.float32
BF16 = jnp.bfloat16
VMEM = pl.BlockSpec(memory_space=pltpu.VMEM)


def ep_index(z, y, c):
    return (z * Y + y) * C + c


EP_ALL = [(z, y, c) for z in range(Z) for y in range(Y) for c in range(C)]
ROW_OFFSETS = (0, -1, 1, 2)
PLANES = [[ep_index(z, y, c) for z in range(Z)] for y in range(Y) for c in range(C)]


def y_perm(d):
    return [(ep_index(z, y, c), ep_index(z, (y + d) % Y, c)) for z, y, c in EP_ALL]


def core_perm():
    return [(ep_index(z, y, c), ep_index(z, y, 1 - c)) for z, y, c in EP_ALL]


def tp_perm(d):
    return [(i, (i + d) % 4) for i in range(4)]


def cost(flops, nbytes):
    return pl.CostEstimate(flops=flops, bytes_accessed=nbytes, transcendentals=0)


def iota(shape, dim):
    return lax.broadcasted_iota(jnp.int32, shape, dim)


def dot(a, b):
    return jnp.dot(a, b, preferred_element_type=F32)


def swap_matrix():
    out_row, in_row = iota((256, 256), 0), iota((256, 256), 1)
    return jnp.where((out_row // SUB == in_row % SUB) & (out_row % SUB == in_row // SUB), 1.0, 0.0).astype(BF16)


def stack_blocks(rows):
    return jnp.concatenate([rows[:, k * 128 : (k + 1) * 128] for k in range(SUB)], axis=0)


def tile_rows(rows32, out_ref, at):
    both = jnp.concatenate([stack_blocks(rows32[:16]), stack_blocks(rows32[16:])], axis=1)
    tiled = dot(swap_matrix(), both).astype(BF16)
    out_ref[at : at + 256, :] = tiled[:, :128]
    out_ref[at + 256 : at + 512, :] = tiled[:, 128:]


def untile_rows(in_ref, at, out_ref, row):
    both = jnp.concatenate([in_ref[at : at + 256, :], in_ref[at + 256 : at + 512, :]], axis=1)
    y = dot(swap_matrix(), both).astype(BF16)
    for k in range(SUB):
        for i in range(2):
            out_ref[row + i * 16 : row + (i + 1) * 16, k * 128 : (k + 1) * 128] = y[
                k * SUB : (k + 1) * SUB, i * 128 : (i + 1) * 128
            ]


def pair_slots(route_row):
    i0, i1 = iota((128, 128), 0), iota((128, 128), 1)
    wide = jnp.broadcast_to(route_row, (128, 128))
    col = jnp.sum(jnp.where(i0 == i1, wide, 0.0), axis=1, keepdims=True)
    same = (jnp.broadcast_to(col, (128, 128)) == wide) & (i0 < i1)
    rank = jnp.sum(jnp.where(same, 1.0, 0.0), axis=0, keepdims=True)
    return route_row * CAP + rank


def prep_kernel(tp_ref, x_ref, gain_ref, route_ref, out_ref):
    x = x_ref[...].astype(F32)
    scale = lax.rsqrt(jnp.mean(x * x, axis=-1, keepdims=True) + 1e-06)
    normed = (x * scale * gain_ref[...].astype(F32)).astype(BF16)
    slots = pair_slots(route_ref[0].astype(F32))
    chosen = jnp.where(
        iota((SLOTS, 128), 0).astype(F32) == jnp.broadcast_to(slots, (SLOTS, 128)), 1.0, 0.0
    ).astype(BF16)
    owner = jnp.where(iota((128, TOK), 0) // 2 == iota((128, TOK), 1), 1.0, 0.0).astype(BF16)
    select = dot(chosen, owner).astype(BF16)
    sent = dot(select, normed).astype(BF16)
    for b in range(SLOTS // 32):
        tile_rows(sent[b * 32 : (b + 1) * 32], out_ref, b * 512)


def prep(tp, routed_input, gain, routes):
    return pl.pallas_call(
        prep_kernel,
        grid_spec=pltpu.PrefetchScalarGridSpec(
            num_scalar_prefetch=1,
            grid=(1,),
            in_specs=[
                pl.BlockSpec((TOK, D), lambda i, tp: (tp[0], 0)),
                pl.BlockSpec((1, D), lambda i, tp: (0, 0)),
                pl.BlockSpec((1, 1, 128), lambda i, tp: (tp[0], 0, 0)),
            ],
            out_specs=pl.BlockSpec((SLOTS * SUB, 128), lambda i, tp: (0, 0)),
        ),
        out_shape=jax.ShapeDtypeStruct((SLOTS * SUB, 128), BF16),
        cost_estimate=cost(400_000_000, 2_000_000),
        name="prep",
    )(tp, routed_input, gain.reshape(1, D), routes.reshape(4, 1, 128))


def untile_kernel(a_ref, o_ref):
    for b in range(SLOTS // 32):
        untile_rows(a_ref, b * 512, o_ref, b * 32)


def untile(a):
    return pl.pallas_call(
        untile_kernel,
        out_shape=jax.ShapeDtypeStruct((SLOTS, D), BF16),
        in_specs=[VMEM],
        out_specs=VMEM,
        cost_estimate=cost(400_000_000, 1_600_000),
        name="untile",
    )(a)


def expert_rows(x, gate_ref, up_ref, down_ref):
    gate = dot(x, gate_ref[0])
    upper = dot(x, up_ref[0])
    hidden = (gate / (1.0 + jnp.exp(-gate)) * upper).astype(BF16)
    return dot(hidden, down_ref[0]).astype(BF16)


def own_kernel(x_ref, gate_ref, up_ref, down_ref, o_ref):
    o_ref[...] = expert_rows(x_ref[...], gate_ref, up_ref, down_ref)


def own_rows(x, weights):
    return pl.pallas_call(
        own_kernel,
        out_shape=jax.ShapeDtypeStruct((SLOTS, D), BF16),
        in_specs=[VMEM] * 4,
        out_specs=VMEM,
        cost_estimate=cost(600_000_000, 1_600_000),
        name="own_rows",
    )(x, *weights)


def halves_kernel(a_ref, b_ref, gate_ref, up_ref, down_ref, a0_ref, a1_ref, b0_ref, b1_ref):
    for x_ref, lo_ref, hi_ref in ((a_ref, a0_ref, a1_ref), (b_ref, b0_ref, b1_ref)):
        y = expert_rows(x_ref[...], gate_ref, up_ref, down_ref)
        lo_ref[...] = y[:TOP]
        hi_ref[...] = y[TOP:]


def halves(a, b, weights):
    return pl.pallas_call(
        halves_kernel,
        out_shape=[jax.ShapeDtypeStruct((TOP, D), BF16)] * 4,
        in_specs=[VMEM] * 5,
        out_specs=[VMEM] * 4,
        cost_estimate=cost(1_200_000_000, 3_200_000),
        name="halves",
    )(a, b, *weights)


def far_kernel(a_ref, b_ref, gate_ref, up_ref, down_ref, a0_ref, b0_ref):
    y = expert_rows(jnp.concatenate([a_ref[...], b_ref[...]], axis=0), gate_ref, up_ref, down_ref)
    a0_ref[...] = y[:TOP]
    b0_ref[...] = y[TOP:]


def far_rows(a, b, weights):
    return pl.pallas_call(
        far_kernel,
        out_shape=[jax.ShapeDtypeStruct((TOP, D), BF16)] * 2,
        in_specs=[VMEM] * 5,
        out_specs=[VMEM] * 2,
        cost_estimate=cost(600_000_000, 1_600_000),
        name="far_rows",
    )(a, b, *weights)


def add_kernel(a_ref, b_ref, c_ref, d_ref, ab_ref, cd_ref):
    ab_ref[...] = (a_ref[...].astype(F32) + b_ref[...].astype(F32)).astype(BF16)
    cd_ref[...] = (c_ref[...].astype(F32) + d_ref[...].astype(F32)).astype(BF16)


def add_pairs(a, b, c, d):
    return pl.pallas_call(
        add_kernel,
        out_shape=[jax.ShapeDtypeStruct((TOP, D), BF16)] * 2,
        in_specs=[VMEM] * 4,
        out_specs=[VMEM] * 2,
        cost_estimate=cost(10_000_000, 2_400_000),
        name="add_pairs",
    )(a, b, c, d)


def total_kernel(own_ref, a0_ref, b0_ref, a1_ref, b1_ref, o_ref):
    for half, a_ref, b_ref in ((0, a0_ref, b0_ref), (1, a1_ref, b1_ref)):
        for b in range(TOP // 32):
            rows = slice(b * 32, (b + 1) * 32)
            at = half * TOP + b * 32
            added = own_ref[at : at + 32, :].astype(F32) + (
                a_ref[rows, :].astype(F32) + b_ref[rows, :].astype(F32)
            )
            tile_rows(added.astype(BF16), o_ref, at * SUB)


def total(*parts):
    return pl.pallas_call(
        total_kernel,
        out_shape=jax.ShapeDtypeStruct((SLOTS * SUB, 128), BF16),
        in_specs=[VMEM] * 5,
        out_specs=VMEM,
        cost_estimate=cost(400_000_000, 3_000_000),
        name="total",
    )(*parts)


def combine_kernel(tp_ref, r_ref, route_ref, weight_ref, o_ref, plain):
    for b in range(SLOTS // 32):
        untile_rows(r_ref, b * 512, plain, b * 32)
    slots = jnp.broadcast_to(pair_slots(route_ref[0].astype(F32)), (TOK, 128))
    pair, token = iota((TOK, 128), 1), iota((TOK, 128), 0)
    added = None
    for k in range(2):
        col = jnp.sum(jnp.where(pair == 2 * token + k, slots, 0.0), axis=1, keepdims=True)
        pick = jnp.where(
            iota((TOK, SLOTS), 1).astype(F32) == jnp.broadcast_to(col, (TOK, SLOTS)), 1.0, 0.0
        ).astype(BF16)
        term = weight_ref[:, k : k + 1] * dot(pick, plain[...])
        added = term if added is None else added + term
    o_ref[...] = added.astype(BF16)


def combine(tp, back, routes, route_weight):
    return pl.pallas_call(
        combine_kernel,
        grid_spec=pltpu.PrefetchScalarGridSpec(
            num_scalar_prefetch=1,
            grid=(1,),
            in_specs=[
                pl.BlockSpec((SLOTS * SUB, 128), lambda i, tp: (0, 0)),
                pl.BlockSpec((1, 1, 128), lambda i, tp: (tp[0], 0, 0)),
                pl.BlockSpec((TOK, 2), lambda i, tp: (tp[0], 0)),
            ],
            out_specs=pl.BlockSpec((TOK, D), lambda i, tp: (0, 0)),
            scratch_shapes=[pltpu.VMEM((SLOTS, D), BF16)],
        ),
        out_shape=jax.ShapeDtypeStruct((TOK, D), BF16),
        cost_estimate=cost(400_000_000, 2_000_000),
        name="combine",
    )(tp, back, routes.reshape(4, 1, 128), route_weight)


def attend_kernel(ep_ref, q_ref, gate_ref, same_ref, other_ref, o_ref, best, total, summed):
    me = ep_ref[0]
    plane, row, core = me // 8, (me // 2) % 4, me % 2
    q = q_ref[...].astype(F32) * 0.125
    q = jnp.concatenate([q[:, :64], q[:, 64:]], axis=0).astype(BF16)
    own_gate = jnp.broadcast_to(gate_ref[:, pl.ds(pl.multiple_of(me * 128, 128), 128)], (128, 128))
    col = jnp.sum(
        jnp.where(iota((128, 128), 0) == iota((128, 128), 1), own_gate, 0.0), axis=1, keepdims=True
    )
    gate_col = jnp.concatenate([col, col], axis=0)

    def blocks_of(z, low, high):
        return jnp.concatenate(
            [ref[z * 4 + i, low:high, :] for ref in (same_ref, other_ref) for i in range(4)], axis=1
        )

    def starts_of(z):
        return [
            ((z * 4 + (row + dy + 4) % 4) * 2 + c) * 128 for c in (core, 1 - core) for dy in ROW_OFFSETS
        ]

    def scores_of(z):
        gates = [gate_ref[:, pl.ds(pl.multiple_of(at, 128), 128)] for at in starts_of(z)]
        return dot(q, blocks_of(z, 0, 64)) + gate_col - jnp.concatenate(gates, axis=1)

    def weighted(weights, z):
        return lax.dot_general(
            weights.astype(BF16),
            blocks_of(z, 64, 128),
            (((1,), (1,)), ((), ())),
            preferred_element_type=F32,
        )

    scores = scores_of(plane)
    query = iota((256, 128), 0) % 128 + me * 128
    allowed = jnp.concatenate([iota((256, 128), 1) + at <= query for at in starts_of(plane)], axis=1)
    scores = jnp.where(allowed, scores, -jnp.inf)
    top = jnp.max(scores, axis=1, keepdims=True)
    weights = jnp.exp(scores - top)
    best[...] = top
    total[...] = jnp.sum(weights, axis=1, keepdims=True)
    summed[...] = weighted(weights, plane)

    @pl.loop(0, plane)
    def _(z):
        scores = scores_of(z)
        before = best[...]
        top = jnp.maximum(before, jnp.max(scores, axis=1, keepdims=True))
        factor = jnp.exp(before - top)
        weights = jnp.exp(scores - top)
        best[...] = top
        total[...] = total[...] * factor + jnp.sum(weights, axis=1, keepdims=True)
        summed[...] = summed[...] * factor + weighted(weights, z)

    out = summed[...] / total[...]
    o_ref[...] = jnp.concatenate([out[:128], out[128:]], axis=1).astype(BF16)


def attend(ep, queries, cum_gate, same, other):
    return pl.pallas_call(
        attend_kernel,
        out_shape=jax.ShapeDtypeStruct((128, 128), BF16),
        in_specs=[pl.BlockSpec(memory_space=pltpu.SMEM)] + [VMEM] * 4,
        out_specs=VMEM,
        scratch_shapes=[
            pltpu.VMEM((256, 1), F32),
            pltpu.VMEM((256, 1), F32),
            pltpu.VMEM((256, 64), F32),
        ],
        cost_estimate=cost(4_000_000_000, 2_500_000),
        name="attend",
    )(ep, queries, cum_gate, same, other)


def over_experts(x):
    return lax.all_to_all(x.reshape(EXPERTS, 48, 128), "ep", 0, 0, tiled=True).reshape(SLOTS * SUB, 128)


def over_planes(own):
    return lax.all_to_all(
        jnp.broadcast_to(own[None], (Z, 4, 128, 128)),
        "ep",
        0,
        0,
        tiled=True,
        axis_index_groups=PLANES,
    ).reshape(32, 128, 128)


def gather_kv(key_cache, value_cache):
    kv = jnp.concatenate([key_cache[0], value_cache[0]], axis=0)
    own = jnp.stack(
        [kv, lax.ppermute(kv, "ep", y_perm(1)), lax.ppermute(kv, "ep", y_perm(-1)), lax.ppermute(kv, "ep", y_perm(2))]
    )
    same = over_planes(own)
    return same, lax.ppermute(same, "ep", core_perm())


def body(
    queries,
    key_cache,
    value_cache,
    cum_gate,
    out_weight,
    routed_input,
    norm_gain,
    routes,
    route_weight,
    expert_gate,
    expert_up,
    expert_down,
):
    tp = lax.axis_index("tp").astype(jnp.int32).reshape(1)
    ep = lax.axis_index("ep").astype(jnp.int32).reshape(1)
    weights = (expert_gate, expert_up, expert_down)
    came = over_experts(prep(tp, routed_input, norm_gain, routes))
    own = untile(came)
    left = lax.ppermute(own, "tp", tp_perm(1))
    right = lax.ppermute(own, "tp", tp_perm(-1))
    far_top = lax.ppermute(left[:TOP], "tp", tp_perm(1))
    far_bottom = lax.ppermute(right[TOP:], "tp", tp_perm(-1))
    own_part = own_rows(own, weights)
    left_top, left_bottom, right_top, right_bottom = halves(left, right, weights)
    far_top, far_bottom = far_rows(far_top, far_bottom, weights)
    mine_top = lax.ppermute(left_top, "tp", tp_perm(-1))
    mine_bottom = lax.ppermute(right_bottom, "tp", tp_perm(1))
    over_top = lax.ppermute(far_top, "tp", tp_perm(1))
    over_bottom = lax.ppermute(far_bottom, "tp", tp_perm(-1))
    right_top, left_bottom = add_pairs(right_top, over_top, left_bottom, over_bottom)
    also_top = lax.ppermute(right_top, "tp", tp_perm(1))
    also_bottom = lax.ppermute(left_bottom, "tp", tp_perm(-1))
    mine = total(own_part, mine_top, also_top, mine_bottom, also_bottom)
    expert_out = combine(tp, over_experts(mine), routes, route_weight)

    same, other = gather_kv(key_cache, value_cache)
    attended = attend(ep, queries, cum_gate, same, other)
    by_position = lax.all_to_all(attended, "tp", split_axis=0, concat_axis=1, tiled=True)
    mixed_out = jnp.dot(by_position, out_weight, preferred_element_type=F32).astype(BF16)
    return (mixed_out, expert_out)


def solution(mesh):
    return jax.shard_map(
        body,
        mesh=mesh,
        in_specs=(
            P("ep", "tp"),
            P("tp", None, "ep"),
            P("tp", None, "ep"),
            P("tp", None),
            P(),
            P("ep", None),
            P(),
            P("ep", None),
            P("ep", None),
            P("ep", None, "tp"),
            P("ep", None, "tp"),
            P("ep", "tp", None),
        ),
        out_specs=(P(("ep", "tp"), None), P(("ep", "tp"), None)),
        check_vma=False,
    )
```

```python
import functools

import jax
import jax.numpy as jnp
from jax import lax
from jax.experimental import pallas as pl
from jax.experimental.pallas import tpu as pltpu
from jax.sharding import PartitionSpec as P


Z, Y, C = 8, 4, 2
TOK = 64
CAP = 3
EXPERTS = 64
SLOTS = EXPERTS * CAP
D = 2048
SUB = 16
TOP = 96
F32 = jnp.float32
BF16 = jnp.bfloat16
VMEM = pl.BlockSpec(memory_space=pltpu.VMEM)
SMEM = pl.BlockSpec(memory_space=pltpu.SMEM)
HBM = pl.BlockSpec(memory_space=pltpu.HBM)
LIMIT = pltpu.CompilerParams(vmem_limit_bytes=12 * 1024 * 1024)


def ep_index(z, y, c):
    return (z * Y + y) * C + c


EP_ALL = [(z, y, c) for z in range(Z) for y in range(Y) for c in range(C)]
ROW_OFFSETS = (0, -1, 1, 2)
TP_SHIFTS = (0, 1, -1, 2)
PLANES = [[ep_index(z, y, c) for z in range(Z)] for y in range(Y) for c in range(C)]


def y_perm(d):
    return [(ep_index(z, y, c), ep_index(z, (y + d) % Y, c)) for z, y, c in EP_ALL]


def core_perm():
    return [(ep_index(z, y, c), ep_index(z, y, 1 - c)) for z, y, c in EP_ALL]


def tp_perm(d):
    return [(i, (i + d) % 4) for i in range(4)]


def cost(flops, nbytes):
    return pl.CostEstimate(flops=flops, bytes_accessed=nbytes, transcendentals=0)


def near(x):
    return pltpu.with_memory_space_constraint(x, pltpu.VMEM)


def near_out(shape, dtype=BF16):
    return pltpu.VMEM(shape, dtype)


def iota(shape, dim):
    return lax.broadcasted_iota(jnp.int32, shape, dim)


def dot(a, b):
    return jnp.dot(a, b, preferred_element_type=F32)


def swap_matrix():
    out_row, in_row = iota((256, 256), 0), iota((256, 256), 1)
    return jnp.where((out_row // SUB == in_row % SUB) & (out_row % SUB == in_row // SUB), 1.0, 0.0).astype(BF16)


def stack_blocks(rows):
    return jnp.concatenate([rows[:, k * 128 : (k + 1) * 128] for k in range(SUB)], axis=0)


def tile_rows(rows, scratch, out_hbm, sems):
    copies = []
    for part in range(3):
        groups = range(part * 4, part * 4 + 4)
        wide = jnp.concatenate([stack_blocks(rows[g * 16 : (g + 1) * 16]) for g in groups], axis=1)
        tiled = dot(swap_matrix(), wide).astype(BF16)
        for i, g in enumerate(groups):
            scratch[g * 256 : (g + 1) * 256, :] = tiled[:, i * 128 : (i + 1) * 128]
        here = pl.ds(part * 1024, 1024)
        copies.append(pltpu.make_async_copy(scratch.at[here, :], out_hbm.at[here, :], sems.at[part]))
        copies[-1].start()
    for copy in copies:
        copy.wait()


def untile_groups(in_ref, groups, place):
    wide = jnp.concatenate([in_ref[g * 256 : (g + 1) * 256, :] for g in groups], axis=1)
    y = dot(swap_matrix(), wide).astype(BF16)
    for i, g in enumerate(groups):
        ref, row = place(g)
        for k in range(SUB):
            ref[row : row + 16, k * 128 : (k + 1) * 128] = y[k * SUB : (k + 1) * SUB, i * 128 : (i + 1) * 128]


TILES = [pltpu.VMEM((SLOTS * SUB, 128), BF16), pltpu.SemaphoreType.DMA((3,))]


def own_lanes(ref, tp):
    whole = ref[...].astype(F32)
    return sum(jnp.where(tp == j, whole[:, j * TOK : (j + 1) * TOK], 0.0) for j in range(4))


def column(row):
    n = row.shape[1]
    wide = jnp.broadcast_to(row, (n, n))
    return jnp.sum(jnp.where(iota((n, n), 0) == iota((n, n), 1), wide, 0.0), axis=1, keepdims=True)


def pair_slots(route_ref, tp):
    routes = own_lanes(route_ref, tp)
    row = jnp.concatenate([routes[0:1], routes[1:2]], axis=1)
    wide = jnp.broadcast_to(row, (128, 128))
    same = jnp.broadcast_to(column(row), (128, 128)) == wide
    earlier = iota((128, 128), 0) % TOK < iota((128, 128), 1) % TOK
    rank = jnp.sum(jnp.where(same & earlier, 1.0, 0.0), axis=0, keepdims=True)
    return row * CAP + rank


def prep_kernel(tp_ref, x_hbm, gain_hbm, route_hbm, out_hbm, x_ref, gain_ref, route_ref, loaded, scratch, sems):
    tp = tp_ref[0]
    mine = x_hbm.at[pl.ds(pl.multiple_of(tp * TOK, TOK), TOK), :]
    pairs = ((route_hbm, route_ref), (mine, x_ref), (gain_hbm, gain_ref))
    copies = [pltpu.make_async_copy(here, there, loaded.at[i]) for i, (here, there) in enumerate(pairs)]
    for copy in copies:
        copy.start()
    copies[0].wait()
    slots = jnp.broadcast_to(pair_slots(route_ref, tp), (SLOTS, 128))
    chosen = jnp.where(iota((SLOTS, 128), 0).astype(F32) == slots, 1.0, 0.0)
    select = (chosen[:, :TOK] + chosen[:, TOK:]).astype(BF16)
    copies[1].wait()
    copies[2].wait()
    x = x_ref[...].astype(F32)
    scale = lax.rsqrt(jnp.mean(x * x, axis=-1, keepdims=True) + 1e-06)
    normed = (x * scale * gain_ref[...].astype(F32).reshape(1, D)).astype(BF16)
    tile_rows(dot(select, normed).astype(BF16), scratch, out_hbm, sems)


def prep(tp, routed_input, gain, routes):
    return pl.pallas_call(
        prep_kernel,
        in_specs=[SMEM, HBM, HBM, HBM],
        out_specs=HBM,
        out_shape=pltpu.HBM((SLOTS * SUB, 128), BF16),
        scratch_shapes=[
            pltpu.VMEM((TOK, D), BF16),
            pltpu.VMEM((D,), BF16),
            pltpu.VMEM((2, 4 * TOK), jnp.int32),
            pltpu.SemaphoreType.DMA((3,)),
        ]
        + TILES,
        cost_estimate=cost(400_000_000, 2_000_000),
        name="prep",
        compiler_params=LIMIT,
    )(tp, *(pltpu.with_memory_space_constraint(x, pltpu.HBM) for x in (routed_input, gain, routes.T)))


def untile_kernel(a_hbm, top_ref, bottom_ref, scratch, sems):
    copies = []
    for part in range(3):
        here = pl.ds(part * 1024, 1024)
        copies.append(pltpu.make_async_copy(a_hbm.at[here, :], scratch.at[here, :], sems.at[part]))
        copies[-1].start()
    for part in range(3):
        copies[part].wait()
        untile_groups(
            scratch,
            range(part * 4, part * 4 + 4),
            lambda g: (top_ref, g * 16) if g < TOP // 16 else (bottom_ref, g * 16 - TOP),
        )


def untile(a):
    return pl.pallas_call(
        untile_kernel,
        out_shape=[near_out((TOP, D))] * 2,
        in_specs=[HBM],
        out_specs=[VMEM] * 2,
        scratch_shapes=TILES,
        cost_estimate=cost(400_000_000, 1_600_000),
        name="untile",
        compiler_params=LIMIT,
    )(pltpu.with_memory_space_constraint(a, pltpu.HBM))


def rows_kernel(count, *refs):
    blocks, (gate_ref, up_ref, down_ref), outs = refs[: -count - 3], refs[-count - 3 : -count], refs[-count:]
    x = jnp.concatenate([ref[...] for ref in blocks], axis=0)
    gate = dot(x, gate_ref[0])
    upper = dot(x, up_ref[0])
    hidden = (gate / (1.0 + jnp.exp(-gate)) * upper).astype(BF16)
    result = dot(hidden, down_ref[0]).astype(BF16)
    rows = result.shape[0] // count
    for i, out in enumerate(outs):
        out[...] = result[i * rows : (i + 1) * rows]


def expert_rows(weights, places, *blocks):
    rows = sum(b.shape[0] for b in blocks)
    count = len(places)
    return pl.pallas_call(
        functools.partial(rows_kernel, count),
        out_shape=[place((rows // count, D), BF16) for place in places],
        in_specs=[VMEM] * (len(blocks) + 3),
        out_specs=[VMEM] * count,
        cost_estimate=cost(3_000_000 * rows, 8_000 * rows),
        name="expert_rows",
        compiler_params=LIMIT,
    )(*(near(b) for b in blocks), *weights)


def add_kernel(a_ref, b_ref, c_ref, d_ref, ab_ref, cd_ref):
    ab_ref[...] = (a_ref[...].astype(F32) + b_ref[...].astype(F32)).astype(BF16)
    cd_ref[...] = (c_ref[...].astype(F32) + d_ref[...].astype(F32)).astype(BF16)


def add_pairs(kept_a, came_a, kept_b, came_b):
    return pl.pallas_call(
        add_kernel,
        out_shape=[near_out((TOP, D))] * 2,
        in_specs=[VMEM] * 4,
        out_specs=[VMEM] * 2,
        cost_estimate=cost(10_000_000, 2_400_000),
        name="add_pairs",
        compiler_params=LIMIT,
    )(kept_a, near(came_a), kept_b, near(came_b))


def total_kernel(own_ref, a0_ref, b0_ref, a1_ref, b1_ref, out_hbm, scratch, sems):
    added = [
        own_ref[i * TOP : (i + 1) * TOP, :].astype(F32) + (a_ref[...].astype(F32) + b_ref[...].astype(F32))
        for i, (a_ref, b_ref) in enumerate(((a0_ref, b0_ref), (a1_ref, b1_ref)))
    ]
    tile_rows(jnp.concatenate(added, axis=0).astype(BF16), scratch, out_hbm, sems)


def total(*parts):
    return pl.pallas_call(
        total_kernel,
        out_shape=pltpu.HBM((SLOTS * SUB, 128), BF16),
        in_specs=[VMEM] * 5,
        out_specs=HBM,
        scratch_shapes=TILES,
        cost_estimate=cost(400_000_000, 3_000_000),
        name="total",
        compiler_params=LIMIT,
    )(parts[0], *(near(p) for p in parts[1:]))


def combine_kernel(tp_ref, r_ref, route_ref, weight_ref, o_ref, plain):
    tp = tp_ref[0]
    slots = pair_slots(route_ref, tp)
    weights = own_lanes(weight_ref, tp)
    for part in range(3):
        untile_groups(r_ref, range(part * 4, part * 4 + 4), lambda g: (plain, g * 16))
    added = None
    for k in range(2):
        slot = jnp.broadcast_to(column(slots[:, k * TOK : (k + 1) * TOK]), (TOK, SLOTS))
        pick = jnp.where(iota((TOK, SLOTS), 1).astype(F32) == slot, 1.0, 0.0).astype(BF16)
        term = column(weights[k : k + 1]) * dot(pick, plain[...])
        added = term if added is None else added + term
    o_ref[...] = added.astype(BF16)


def combine(tp, back, routes, route_weight):
    return pl.pallas_call(
        combine_kernel,
        in_specs=[SMEM, VMEM, VMEM, VMEM],
        out_specs=VMEM,
        out_shape=jax.ShapeDtypeStruct((TOK, D), BF16),
        scratch_shapes=[pltpu.VMEM((SLOTS, D), BF16)],
        cost_estimate=cost(400_000_000, 2_000_000),
        name="combine",
        compiler_params=LIMIT,
    )(tp, near(back), routes.T, route_weight.T)


def attend_kernel(last, ep_ref, tp_ref, q_ref, gate_ref, blocks_ref, *refs):
    carried, refs = (refs[:3], refs[3:]) if last else ((), refs)
    outs, (best, total, summed, out_ref) = (refs[:4], refs[4:]) if last else ((), refs + (None,))
    me = ep_ref[0]
    plane, row, core = me // 8, (me // 2) % 4, me % 2
    core = 1 - core if last else core
    q = q_ref[...].astype(F32) * 0.125
    q = jnp.concatenate([q[:, :64], q[:, 64:]], axis=0).astype(BF16)
    col = column(gate_ref[:, pl.ds(pl.multiple_of(me * 128, 128), 128)])
    gate_col = jnp.concatenate([col, col], axis=0)

    def blocks_of(z, low, high):
        return jnp.concatenate([blocks_ref[z * 4 + i, low:high, :] for i in range(4)], axis=1)

    def starts_of(z):
        return [((z * 4 + (row + dy + 4) % 4) * 2 + core) * 128 for dy in ROW_OFFSETS]

    def scores_of(z):
        gates = [gate_ref[:, pl.ds(pl.multiple_of(at, 128), 128)] for at in starts_of(z)]
        return dot(q, blocks_of(z, 0, 64)) + gate_col - jnp.concatenate(gates, axis=1)

    def weighted(weights, z):
        return lax.dot_general(
            weights.astype(BF16),
            blocks_of(z, 64, 128),
            (((1,), (1,)), ((), ())),
            preferred_element_type=F32,
        )

    def merge(scores, z, before, count, product):
        top = jnp.maximum(before, jnp.max(scores, axis=1, keepdims=True))
        factor = jnp.exp(before - top)
        weights = jnp.exp(scores - top)
        best[...] = top
        total[...] = count * factor + jnp.sum(weights, axis=1, keepdims=True)
        summed[...] = product * factor + weighted(weights, z)

    scores = scores_of(plane)
    query = iota((256, 128), 0) % 128 + me * 128
    allowed = jnp.concatenate([iota((256, 128), 1) + at <= query for at in starts_of(plane)], axis=1)
    scores = jnp.where(allowed, scores, -jnp.inf)
    if last:
        merge(scores, plane, *(ref[...] for ref in carried))
    else:
        top = jnp.max(scores, axis=1, keepdims=True)
        weights = jnp.exp(scores - top)
        best[...] = top
        total[...] = jnp.sum(weights, axis=1, keepdims=True)
        summed[...] = weighted(weights, plane)

    @pl.loop(0, plane)
    def _(z):
        merge(scores_of(z), z, best[...], total[...], summed[...])

    if last:
        out = summed[...] / total[...]
        out_ref[...] = jnp.concatenate([out[:128], out[128:]], axis=1)
        for ref, shift in zip(outs, TP_SHIFTS):
            at = pl.multiple_of((tp_ref[0] + shift + 4) % 4 * 32, 32)
            ref[...] = out_ref[pl.ds(at, 32), :].astype(BF16)


STATE = ((256, 1), (256, 1), (256, 64))


def attend_same(ep, tp, queries, cum_gate, blocks):
    return pl.pallas_call(
        functools.partial(attend_kernel, False),
        out_shape=[near_out(shape, F32) for shape in STATE],
        in_specs=[SMEM] * 2 + [VMEM] * 3,
        out_specs=[VMEM] * 3,
        cost_estimate=cost(2_000_000_000, 1_500_000),
        name="attend_same",
        compiler_params=LIMIT,
    )(ep, tp, near(queries), near(cum_gate), near(blocks))


def attend_other(ep, tp, queries, cum_gate, blocks, state):
    return pl.pallas_call(
        functools.partial(attend_kernel, True),
        out_shape=[near_out((32, 128))] * 4,
        in_specs=[SMEM] * 2 + [VMEM] * 6,
        out_specs=[VMEM] * 4,
        scratch_shapes=[pltpu.VMEM(shape, F32) for shape in STATE + ((128, 128),)],
        cost_estimate=cost(2_000_000_000, 1_500_000),
        name="attend_other",
        compiler_params=LIMIT,
    )(ep, tp, near(queries), near(cum_gate), near(blocks), *(near(x) for x in state))


def project_kernel(tp_ref, a_ref, b_ref, c_ref, d_ref, w_ref, o_ref):
    added = None
    for ref, shift in zip((a_ref, b_ref, c_ref, d_ref), TP_SHIFTS):
        at = pl.multiple_of((tp_ref[0] - shift + 4) % 4 * 128, 128)
        term = dot(ref[...], w_ref[pl.ds(at, 128), :])
        added = term if added is None else added + term
    o_ref[...] = added.astype(BF16)


def project(tp, parts, out_weight):
    return pl.pallas_call(
        project_kernel,
        out_shape=jax.ShapeDtypeStruct((32, D), BF16),
        in_specs=[SMEM] + [VMEM] * 5,
        out_specs=VMEM,
        cost_estimate=cost(70_000_000, 2_300_000),
        name="project",
        compiler_params=LIMIT,
    )(tp, *(near(p) for p in parts), out_weight)


def over_experts(x):
    return lax.all_to_all(x.reshape(EXPERTS, 48, 128), "ep", 0, 0, tiled=True).reshape(SLOTS * SUB, 128)


def repeat_kernel(a_ref, b_ref, c_ref, d_ref, o_ref):
    for i, ref in enumerate((a_ref, b_ref, c_ref, d_ref)):
        for z in range(Z):
            o_ref[z, i] = ref[...]


def repeated(*blocks):
    return pl.pallas_call(
        repeat_kernel,
        out_shape=pltpu.HBM((Z, 4, 128, 128), BF16),
        in_specs=[VMEM] * 4,
        out_specs=VMEM,
        cost_estimate=cost(1_000_000, 1_200_000),
        name="repeat",
        compiler_params=LIMIT,
    )(*(near(b) for b in blocks))


def over_planes(own):
    return lax.all_to_all(own, "ep", 0, 0, tiled=True, axis_index_groups=PLANES).reshape(32, 128, 128)


def gather_kv(key_cache, value_cache):
    kv = jnp.concatenate([key_cache[0], value_cache[0]], axis=0)
    ring = repeated(
        kv, lax.ppermute(kv, "ep", y_perm(1)), lax.ppermute(kv, "ep", y_perm(-1)), lax.ppermute(kv, "ep", y_perm(2))
    )
    same = over_planes(ring)
    return same, lax.ppermute(same, "ep", core_perm())


def body(
    queries,
    key_cache,
    value_cache,
    cum_gate,
    out_weight,
    routed_input,
    norm_gain,
    routes,
    route_weight,
    expert_gate,
    expert_up,
    expert_down,
):
    tp = lax.axis_index("tp").astype(jnp.int32).reshape(1)
    ep = lax.axis_index("ep").astype(jnp.int32).reshape(1)
    weights = (near(expert_gate), near(expert_up), near(expert_down))
    came = over_experts(prep(tp, routed_input, norm_gain, routes))
    own_top, own_bottom = untile(came)
    left_top = lax.ppermute(own_top, "tp", tp_perm(1))
    right_bottom = lax.ppermute(own_bottom, "tp", tp_perm(-1))
    left_bottom = lax.ppermute(own_bottom, "tp", tp_perm(1))
    right_top = lax.ppermute(own_top, "tp", tp_perm(-1))
    far_top = lax.ppermute(left_top, "tp", tp_perm(1))
    far_bottom = lax.ppermute(right_bottom, "tp", tp_perm(-1))
    (own_part,) = expert_rows(weights, (pltpu.HBM,), own_top, own_bottom)
    left_part_top, left_part_bottom, right_part_top, right_part_bottom = expert_rows(
        weights, (pltpu.VMEM, pltpu.HBM, pltpu.HBM, pltpu.VMEM), left_top, left_bottom, right_top, right_bottom
    )
    far_part_top, far_part_bottom = expert_rows(weights, (pltpu.VMEM,) * 2, far_top, far_bottom)
    from_right_top = lax.ppermute(left_part_top, "tp", tp_perm(-1))
    from_left_bottom = lax.ppermute(right_part_bottom, "tp", tp_perm(1))
    passed_top = lax.ppermute(far_part_top, "tp", tp_perm(1))
    passed_bottom = lax.ppermute(far_part_bottom, "tp", tp_perm(-1))
    right_part_top, left_part_bottom = add_pairs(right_part_top, passed_top, left_part_bottom, passed_bottom)
    from_left_top = lax.ppermute(right_part_top, "tp", tp_perm(1))
    from_right_bottom = lax.ppermute(left_part_bottom, "tp", tp_perm(-1))
    mine = total(own_part, from_right_top, from_left_top, from_left_bottom, from_right_bottom)
    expert_out = combine(tp, over_experts(mine), routes, route_weight)

    same, other = gather_kv(key_cache, value_cache)
    state = attend_same(ep, tp, queries, cum_gate, same)
    rows, up, down, across = attend_other(ep, tp, queries, cum_gate, other, state)
    parts = (
        rows,
        lax.ppermute(up, "tp", tp_perm(1)),
        lax.ppermute(down, "tp", tp_perm(-1)),
        lax.ppermute(across, "tp", tp_perm(2)),
    )
    mixed_out = project(tp, parts, out_weight)
    return (mixed_out, expert_out)


def solution(mesh):
    return jax.shard_map(
        body,
        mesh=mesh,
        in_specs=(
            P("ep", "tp"),
            P("tp", None, "ep"),
            P("tp", None, "ep"),
            P("tp", None),
            P(),
            P("ep", None),
            P(),
            P("ep", None),
            P("ep", None),
            P("ep", None, "tp"),
            P("ep", None, "tp"),
            P("ep", "tp", None),
        ),
        out_specs=(P(("ep", "tp"), None), P(("ep", "tp"), None)),
        check_vma=False,
    )
```

```python
import functools

import jax
import jax.numpy as jnp
from jax import lax
from jax.experimental import pallas as pl
from jax.experimental.pallas import tpu as pltpu
from jax.sharding import PartitionSpec as P


Z, Y, C = 8, 4, 2
TOK = 64
CAP = 3
EXPERTS = 64
SLOTS = EXPERTS * CAP
D = 2048
SUB = 16
TOP = 96
QUARTER = 48
F32 = jnp.float32
BF16 = jnp.bfloat16
VMEM = pl.BlockSpec(memory_space=pltpu.VMEM)
SMEM = pl.BlockSpec(memory_space=pltpu.SMEM)
HBM = pl.BlockSpec(memory_space=pltpu.HBM)
LIMIT = pltpu.CompilerParams(vmem_limit_bytes=12 * 1024 * 1024)


def ep_index(z, y, c):
    return (z * Y + y) * C + c


EP_ALL = [(z, y, c) for z in range(Z) for y in range(Y) for c in range(C)]
ROW_OFFSETS = (0, -1, 1, 2)
TP_SHIFTS = (0, 1, -1, 2)
PLANES = [[ep_index(z, y, c) for z in range(Z)] for y in range(Y) for c in range(C)]


def y_perm(d):
    return [(ep_index(z, y, c), ep_index(z, (y + d) % Y, c)) for z, y, c in EP_ALL]


def core_perm():
    return [(ep_index(z, y, c), ep_index(z, y, 1 - c)) for z, y, c in EP_ALL]


def tp_perm(d):
    return [(i, (i + d) % 4) for i in range(4)]


def cost(flops, nbytes):
    return pl.CostEstimate(flops=flops, bytes_accessed=nbytes, transcendentals=0)


def near(x):
    return pltpu.with_memory_space_constraint(x, pltpu.VMEM)


def near_out(shape, dtype=BF16):
    return pltpu.VMEM(shape, dtype)


def iota(shape, dim):
    return lax.broadcasted_iota(jnp.int32, shape, dim)


def dot(a, b):
    return jnp.dot(a, b, preferred_element_type=F32)


def swap_matrix():
    out_row, in_row = iota((256, 256), 0), iota((256, 256), 1)
    return jnp.where((out_row // SUB == in_row % SUB) & (out_row % SUB == in_row // SUB), 1.0, 0.0).astype(BF16)


def stack_blocks(rows):
    return jnp.concatenate([rows[:, k * 128 : (k + 1) * 128] for k in range(SUB)], axis=0)


def tile_rows(rows, groups, scratch, out_hbm, sem):
    wide = jnp.concatenate([stack_blocks(rows[i * 16 : (i + 1) * 16]) for i in range(len(groups))], axis=1)
    tiled = dot(swap_matrix(), wide).astype(BF16)
    for i, g in enumerate(groups):
        scratch[g * 256 : (g + 1) * 256, :] = tiled[:, i * 128 : (i + 1) * 128]
    here = pl.ds(groups[0] * 256, len(groups) * 256)
    copy = pltpu.make_async_copy(scratch.at[here, :], out_hbm.at[here, :], sem)
    copy.start()
    return copy


def untile_groups(in_ref, groups, place):
    wide = jnp.concatenate([in_ref[g * 256 : (g + 1) * 256, :] for g in groups], axis=1)
    y = dot(swap_matrix(), wide).astype(BF16)
    for i, g in enumerate(groups):
        ref, row = place(g)
        for k in range(SUB):
            ref[row : row + 16, k * 128 : (k + 1) * 128] = y[k * SUB : (k + 1) * SUB, i * 128 : (i + 1) * 128]


TILES = [pltpu.VMEM((SLOTS * SUB, 128), BF16), pltpu.SemaphoreType.DMA((3,))]


def own_lanes(ref, tp):
    whole = ref[...].astype(F32)
    return sum(jnp.where(tp == j, whole[:, j * TOK : (j + 1) * TOK], 0.0) for j in range(4))


def column(row):
    n = row.shape[1]
    wide = jnp.broadcast_to(row, (n, n))
    return jnp.sum(jnp.where(iota((n, n), 0) == iota((n, n), 1), wide, 0.0), axis=1, keepdims=True)


def pair_slots(route_ref, tp):
    routes = own_lanes(route_ref, tp)
    row = jnp.concatenate([routes[0:1], routes[1:2]], axis=1)
    wide = jnp.broadcast_to(row, (128, 128))
    same = jnp.broadcast_to(column(row), (128, 128)) == wide
    earlier = iota((128, 128), 0) % TOK < iota((128, 128), 1) % TOK
    rank = jnp.sum(jnp.where(same & earlier, 1.0, 0.0), axis=0, keepdims=True)
    return row * CAP + rank


def prep_kernel(tp_ref, x_hbm, gain_hbm, route_hbm, out_hbm, x_ref, gain_ref, route_ref, loaded, scratch, sems):
    tp = tp_ref[0]
    mine = x_hbm.at[pl.ds(pl.multiple_of(tp * TOK, TOK), TOK), :]
    pairs = ((route_hbm, route_ref), (mine, x_ref), (gain_hbm, gain_ref))
    copies = [pltpu.make_async_copy(here, there, loaded.at[i]) for i, (here, there) in enumerate(pairs)]
    for copy in copies:
        copy.start()
    copies[0].wait()
    slots = jnp.broadcast_to(pair_slots(route_ref, tp), (SLOTS, 128))
    chosen = jnp.where(iota((SLOTS, 128), 0).astype(F32) == slots, 1.0, 0.0)
    select = (chosen[:, :TOK] + chosen[:, TOK:]).astype(BF16)
    copies[1].wait()
    copies[2].wait()
    x = x_ref[...].astype(F32)
    scale = lax.rsqrt(jnp.mean(x * x, axis=-1, keepdims=True) + 1e-06)
    normed = (x * scale * gain_ref[...].astype(F32).reshape(1, D)).astype(BF16)
    sent = dot(select, normed).astype(BF16)
    copies = [
        tile_rows(sent[part * 64 : (part + 1) * 64], range(part * 4, part * 4 + 4), scratch, out_hbm, sems.at[part])
        for part in range(3)
    ]
    for copy in copies:
        copy.wait()


def prep(tp, routed_input, gain, routes):
    return pl.pallas_call(
        prep_kernel,
        in_specs=[SMEM, HBM, HBM, HBM],
        out_specs=HBM,
        out_shape=pltpu.HBM((SLOTS * SUB, 128), BF16),
        scratch_shapes=[
            pltpu.VMEM((TOK, D), BF16),
            pltpu.VMEM((D,), BF16),
            pltpu.VMEM((2, 4 * TOK), jnp.int32),
            pltpu.SemaphoreType.DMA((3,)),
        ]
        + TILES,
        cost_estimate=cost(400_000_000, 2_000_000),
        name="prep",
        compiler_params=LIMIT,
    )(tp, *(pltpu.with_memory_space_constraint(x, pltpu.HBM) for x in (routed_input, gain, routes.T)))


def untile_kernel(a_hbm, top_ref, bottom_ref, scratch, sems):
    copies = []
    for part in range(3):
        here = pl.ds(part * 1024, 1024)
        copies.append(pltpu.make_async_copy(a_hbm.at[here, :], scratch.at[here, :], sems.at[part]))
        copies[-1].start()
    for part in range(3):
        copies[part].wait()
        untile_groups(
            scratch,
            range(part * 4, part * 4 + 4),
            lambda g: (top_ref, g * 16) if g < TOP // 16 else (bottom_ref, g * 16 - TOP),
        )


def untile(a):
    return pl.pallas_call(
        untile_kernel,
        out_shape=[near_out((TOP, D))] * 2,
        in_specs=[HBM],
        out_specs=[VMEM] * 2,
        scratch_shapes=TILES,
        cost_estimate=cost(400_000_000, 1_600_000),
        name="untile",
        compiler_params=LIMIT,
    )(pltpu.with_memory_space_constraint(a, pltpu.HBM))


def rows_kernel(count, *refs):
    blocks, (gate_ref, up_ref, down_ref), outs = refs[: -count - 3], refs[-count - 3 : -count], refs[-count:]
    x = jnp.concatenate([ref[...] for ref in blocks], axis=0)
    gate = dot(x, gate_ref[0])
    upper = dot(x, up_ref[0])
    hidden = (gate / (1.0 + jnp.exp(-gate)) * upper).astype(BF16)
    result = dot(hidden, down_ref[0]).astype(BF16)
    at = 0
    for out in outs:
        out[...] = result[at : at + out.shape[0]]
        at += out.shape[0]


def expert_rows(weights, pieces, *blocks):
    rows = sum(b.shape[0] for b in blocks)
    return pl.pallas_call(
        functools.partial(rows_kernel, len(pieces)),
        out_shape=[place((count, D), BF16) for count, place in pieces],
        in_specs=[VMEM] * (len(blocks) + 3),
        out_specs=[VMEM] * len(pieces),
        cost_estimate=cost(3_000_000 * rows, 8_000 * rows),
        name="expert_rows",
        compiler_params=LIMIT,
    )(*(near(b) for b in blocks), *weights)


def add_kernel(a_ref, b_ref, c_ref, d_ref, ab_ref, cd_ref):
    ab_ref[...] = (a_ref[...].astype(F32) + b_ref[...].astype(F32)).astype(BF16)
    cd_ref[...] = (c_ref[...].astype(F32) + d_ref[...].astype(F32)).astype(BF16)


def add_pairs(kept_a, came_a, kept_b, came_b):
    return pl.pallas_call(
        add_kernel,
        out_shape=[near_out((QUARTER, D))] * 2,
        in_specs=[VMEM] * 4,
        out_specs=[VMEM] * 2,
        cost_estimate=cost(10_000_000, 1_200_000),
        name="add_pairs",
        compiler_params=LIMIT,
    )(kept_a, near(came_a), kept_b, near(came_b))


def total1_kernel(own_ref, top_ref, bottom_ref, top1_ref, bottom1_ref, out_hbm, sum_ref, scratch, sems):
    copies = []
    for half, (early, late) in enumerate(((top_ref, top1_ref), (bottom_ref, bottom1_ref))):
        first = slice(half * TOP, half * TOP + QUARTER)
        second = slice(half * TOP + QUARTER, (half + 1) * TOP)
        added = own_ref[first, :].astype(F32) + (early[:QUARTER, :].astype(F32) + late[...].astype(F32))
        copies.append(tile_rows(added.astype(BF16), range(half * 6, half * 6 + 3), scratch, out_hbm, sems.at[half]))
        sum_ref[half] = own_ref[second, :].astype(F32) + early[QUARTER:, :].astype(F32)
    for copy in copies:
        copy.wait()


def total1(*parts):
    return pl.pallas_call(
        total1_kernel,
        out_shape=[pltpu.HBM((SLOTS * SUB, 128), BF16), near_out((2, QUARTER, D), F32)],
        in_specs=[VMEM] * 5,
        out_specs=[HBM, VMEM],
        scratch_shapes=TILES,
        cost_estimate=cost(200_000_000, 3_000_000),
        name="total1",
        compiler_params=LIMIT,
    )(parts[0], *(near(p) for p in parts[1:]))


def total2_kernel(begun_hbm, sum_ref, top2_ref, bottom2_ref, out_hbm, scratch, sems):
    copies = []
    for half, late in enumerate((top2_ref, bottom2_ref)):
        added = sum_ref[half] + late[...].astype(F32)
        groups = range(half * 6 + 3, half * 6 + 6)
        copies.append(tile_rows(added.astype(BF16), groups, scratch, out_hbm, sems.at[half]))
    for copy in copies:
        copy.wait()


def total2(begun, *parts):
    return pl.pallas_call(
        total2_kernel,
        out_shape=pltpu.HBM((SLOTS * SUB, 128), BF16),
        in_specs=[HBM] + [VMEM] * 3,
        out_specs=HBM,
        scratch_shapes=TILES,
        input_output_aliases={0: 0},
        cost_estimate=cost(200_000_000, 1_500_000),
        name="total2",
        compiler_params=LIMIT,
    )(begun, *(near(p) for p in parts))


def combine_kernel(tp_ref, r_ref, route_ref, weight_ref, o_ref, plain):
    tp = tp_ref[0]
    slots = pair_slots(route_ref, tp)
    weights = own_lanes(weight_ref, tp)
    for part in range(3):
        untile_groups(r_ref, range(part * 4, part * 4 + 4), lambda g: (plain, g * 16))
    added = None
    for k in range(2):
        slot = jnp.broadcast_to(column(slots[:, k * TOK : (k + 1) * TOK]), (TOK, SLOTS))
        pick = jnp.where(iota((TOK, SLOTS), 1).astype(F32) == slot, 1.0, 0.0).astype(BF16)
        term = column(weights[k : k + 1]) * dot(pick, plain[...])
        added = term if added is None else added + term
    o_ref[...] = added.astype(BF16)


def combine(tp, back, routes, route_weight):
    return pl.pallas_call(
        combine_kernel,
        in_specs=[SMEM, VMEM, VMEM, VMEM],
        out_specs=VMEM,
        out_shape=jax.ShapeDtypeStruct((TOK, D), BF16),
        scratch_shapes=[pltpu.VMEM((SLOTS, D), BF16)],
        cost_estimate=cost(400_000_000, 2_000_000),
        name="combine",
        compiler_params=LIMIT,
    )(tp, near(back), routes.T, route_weight.T)


def attend_kernel(last, ep_ref, tp_ref, q_ref, gate_ref, blocks_ref, *refs):
    carried, refs = (refs[:3], refs[3:]) if last else ((), refs)
    outs, (best, total, summed, out_ref) = (refs[:4], refs[4:]) if last else ((), refs + (None,))
    me = ep_ref[0]
    plane, row, core = me // 8, (me // 2) % 4, me % 2
    core = 1 - core if last else core
    q = q_ref[...].astype(F32) * 0.125
    q = jnp.concatenate([q[:, :64], q[:, 64:]], axis=0).astype(BF16)
    col = column(gate_ref[:, pl.ds(pl.multiple_of(me * 128, 128), 128)])
    gate_col = jnp.concatenate([col, col], axis=0)

    def blocks_of(z, low, high):
        return jnp.concatenate([blocks_ref[z * 4 + i, low:high, :] for i in range(4)], axis=1)

    def starts_of(z):
        return [((z * 4 + (row + dy + 4) % 4) * 2 + core) * 128 for dy in ROW_OFFSETS]

    def scores_of(z):
        gates = [gate_ref[:, pl.ds(pl.multiple_of(at, 128), 128)] for at in starts_of(z)]
        return dot(q, blocks_of(z, 0, 64)) + gate_col - jnp.concatenate(gates, axis=1)

    def weighted(weights, z):
        return lax.dot_general(
            weights.astype(BF16),
            blocks_of(z, 64, 128),
            (((1,), (1,)), ((), ())),
            preferred_element_type=F32,
        )

    def merge(scores, z, before, count, product):
        top = jnp.maximum(before, jnp.max(scores, axis=1, keepdims=True))
        factor = jnp.exp(before - top)
        weights = jnp.exp(scores - top)
        best[...] = top
        total[...] = count * factor + jnp.sum(weights, axis=1, keepdims=True)
        summed[...] = product * factor + weighted(weights, z)

    scores = scores_of(plane)
    query = iota((256, 128), 0) % 128 + me * 128
    allowed = jnp.concatenate([iota((256, 128), 1) + at <= query for at in starts_of(plane)], axis=1)
    scores = jnp.where(allowed, scores, -jnp.inf)
    if last:
        merge(scores, plane, *(ref[...] for ref in carried))
    else:
        top = jnp.max(scores, axis=1, keepdims=True)
        weights = jnp.exp(scores - top)
        best[...] = top
        total[...] = jnp.sum(weights, axis=1, keepdims=True)
        summed[...] = weighted(weights, plane)

    @pl.loop(0, plane)
    def _(z):
        merge(scores_of(z), z, best[...], total[...], summed[...])

    if last:
        out = summed[...] / total[...]
        out_ref[...] = jnp.concatenate([out[:128], out[128:]], axis=1)
        for ref, shift in zip(outs, TP_SHIFTS):
            at = pl.multiple_of((tp_ref[0] + shift + 4) % 4 * 32, 32)
            ref[...] = out_ref[pl.ds(at, 32), :].astype(BF16)


STATE = ((256, 1), (256, 1), (256, 64))


def attend_same(ep, tp, queries, cum_gate, blocks):
    return pl.pallas_call(
        functools.partial(attend_kernel, False),
        out_shape=[near_out(shape, F32) for shape in STATE],
        in_specs=[SMEM] * 2 + [VMEM] * 3,
        out_specs=[VMEM] * 3,
        cost_estimate=cost(2_000_000_000, 1_500_000),
        name="attend_same",
        compiler_params=LIMIT,
    )(ep, tp, near(queries), near(cum_gate), near(blocks))


def attend_other(ep, tp, queries, cum_gate, blocks, state):
    return pl.pallas_call(
        functools.partial(attend_kernel, True),
        out_shape=[near_out((32, 128))] * 4,
        in_specs=[SMEM] * 2 + [VMEM] * 6,
        out_specs=[VMEM] * 4,
        scratch_shapes=[pltpu.VMEM(shape, F32) for shape in STATE + ((128, 128),)],
        cost_estimate=cost(2_000_000_000, 1_500_000),
        name="attend_other",
        compiler_params=LIMIT,
    )(ep, tp, near(queries), near(cum_gate), near(blocks), *(near(x) for x in state))


def project_kernel(tp_ref, a_ref, b_ref, c_ref, d_ref, w_ref, o_ref):
    added = None
    for ref, shift in zip((a_ref, b_ref, c_ref, d_ref), TP_SHIFTS):
        at = pl.multiple_of((tp_ref[0] - shift + 4) % 4 * 128, 128)
        term = dot(ref[...], w_ref[pl.ds(at, 128), :])
        added = term if added is None else added + term
    o_ref[...] = added.astype(BF16)


def project(tp, parts, out_weight):
    return pl.pallas_call(
        project_kernel,
        out_shape=jax.ShapeDtypeStruct((32, D), BF16),
        in_specs=[SMEM] + [VMEM] * 5,
        out_specs=VMEM,
        cost_estimate=cost(70_000_000, 2_300_000),
        name="project",
        compiler_params=LIMIT,
    )(tp, *(near(p) for p in parts), out_weight)


def over_experts(x):
    return lax.all_to_all(x.reshape(EXPERTS, 48, 128), "ep", 0, 0, tiled=True).reshape(SLOTS * SUB, 128)


def repeat_kernel(a_ref, b_ref, c_ref, d_ref, o_ref):
    for i, ref in enumerate((a_ref, b_ref, c_ref, d_ref)):
        for z in range(Z):
            o_ref[z, i] = ref[...]


def repeated(*blocks):
    return pl.pallas_call(
        repeat_kernel,
        out_shape=pltpu.HBM((Z, 4, 128, 128), BF16),
        in_specs=[VMEM] * 4,
        out_specs=VMEM,
        cost_estimate=cost(1_000_000, 1_200_000),
        name="repeat",
        compiler_params=LIMIT,
    )(*(near(b) for b in blocks))


def over_planes(own):
    return lax.all_to_all(own, "ep", 0, 0, tiled=True, axis_index_groups=PLANES).reshape(32, 128, 128)


def gather_kv(key_cache, value_cache):
    kv = jnp.concatenate([key_cache[0], value_cache[0]], axis=0)
    ring = repeated(
        kv, lax.ppermute(kv, "ep", y_perm(1)), lax.ppermute(kv, "ep", y_perm(-1)), lax.ppermute(kv, "ep", y_perm(2))
    )
    same = over_planes(ring)
    return same, lax.ppermute(same, "ep", core_perm())


def body(
    queries,
    key_cache,
    value_cache,
    cum_gate,
    out_weight,
    routed_input,
    norm_gain,
    routes,
    route_weight,
    expert_gate,
    expert_up,
    expert_down,
):
    tp = lax.axis_index("tp").astype(jnp.int32).reshape(1)
    ep = lax.axis_index("ep").astype(jnp.int32).reshape(1)
    weights = (near(expert_gate), near(expert_up), near(expert_down))
    came = over_experts(prep(tp, routed_input, norm_gain, routes))
    own_top, own_bottom = untile(came)
    left_top = lax.ppermute(own_top, "tp", tp_perm(1))
    right_bottom = lax.ppermute(own_bottom, "tp", tp_perm(-1))
    left_bottom = lax.ppermute(own_bottom, "tp", tp_perm(1))
    right_top = lax.ppermute(own_top, "tp", tp_perm(-1))
    far_top = lax.ppermute(left_top, "tp", tp_perm(1))
    far_bottom = lax.ppermute(right_bottom, "tp", tp_perm(-1))
    quarter, half = (QUARTER, pltpu.HBM), (TOP, pltpu.VMEM)
    (own_part,) = expert_rows(weights, ((SLOTS, pltpu.HBM),), own_top, own_bottom)
    left_early, left1, left2, right1, right2, right_early = expert_rows(
        weights, (half, quarter, quarter, quarter, quarter, half), left_top, left_bottom, right_top, right_bottom
    )
    top1, top2, bottom1, bottom2 = expert_rows(weights, ((QUARTER, pltpu.VMEM),) * 4, far_top, far_bottom)
    early_top = lax.ppermute(left_early, "tp", tp_perm(-1))
    early_bottom = lax.ppermute(right_early, "tp", tp_perm(1))
    late = []
    for top, bottom, left, right in ((top1, bottom1, left1, right1), (top2, bottom2, left2, right2)):
        passed_top = lax.ppermute(top, "tp", tp_perm(1))
        passed_bottom = lax.ppermute(bottom, "tp", tp_perm(-1))
        right, left = add_pairs(right, passed_top, left, passed_bottom)
        late.append((lax.ppermute(right, "tp", tp_perm(1)), lax.ppermute(left, "tp", tp_perm(-1))))
    (late_top1, late_bottom1), (late_top2, late_bottom2) = late
    mine, sums = total1(own_part, early_top, early_bottom, late_top1, late_bottom1)
    mine = total2(mine, sums, late_top2, late_bottom2)
    expert_out = combine(tp, over_experts(mine), routes, route_weight)

    same, other = gather_kv(key_cache, value_cache)
    state = attend_same(ep, tp, queries, cum_gate, same)
    rows, up, down, across = attend_other(ep, tp, queries, cum_gate, other, state)
    parts = (
        rows,
        lax.ppermute(up, "tp", tp_perm(1)),
        lax.ppermute(down, "tp", tp_perm(-1)),
        lax.ppermute(across, "tp", tp_perm(2)),
    )
    mixed_out = project(tp, parts, out_weight)
    return (mixed_out, expert_out)


def solution(mesh):
    return jax.shard_map(
        body,
        mesh=mesh,
        in_specs=(
            P("ep", "tp"),
            P("tp", None, "ep"),
            P("tp", None, "ep"),
            P("tp", None),
            P(),
            P("ep", None),
            P(),
            P("ep", None),
            P("ep", None),
            P("ep", None, "tp"),
            P("ep", None, "tp"),
            P("ep", "tp", None),
        ),
        out_specs=(P(("ep", "tp"), None), P(("ep", "tp"), None)),
        check_vma=False,
    )
```

```python
import functools

import jax
import jax.numpy as jnp
from jax import lax
from jax.experimental import pallas as pl
from jax.experimental.pallas import tpu as pltpu
from jax.sharding import PartitionSpec as P


Z, Y, C = 8, 4, 2
TOK = 64
CAP = 3
EXPERTS = 64
SLOTS = EXPERTS * CAP
D = 2048
SUB = 16
TOP = 96
QUARTER = 48
F32 = jnp.float32
BF16 = jnp.bfloat16
VMEM = pl.BlockSpec(memory_space=pltpu.VMEM)
SMEM = pl.BlockSpec(memory_space=pltpu.SMEM)
HBM = pl.BlockSpec(memory_space=pltpu.HBM)
LIMIT = pltpu.CompilerParams(vmem_limit_bytes=12 * 1024 * 1024)


def ep_index(z, y, c):
    return (z * Y + y) * C + c


EP_ALL = [(z, y, c) for z in range(Z) for y in range(Y) for c in range(C)]
ROW_OFFSETS = (0, -1, 1, 2)
TP_SHIFTS = (0, 1, -1, 2)
PLANES = [[ep_index(z, y, c) for z in range(Z)] for y in range(Y) for c in range(C)]


def y_perm(d):
    return [(ep_index(z, y, c), ep_index(z, (y + d) % Y, c)) for z, y, c in EP_ALL]


def core_perm():
    return [(ep_index(z, y, c), ep_index(z, y, 1 - c)) for z, y, c in EP_ALL]


def tp_perm(d):
    return [(i, (i + d) % 4) for i in range(4)]


def ring_perm(d):
    return [
        (e * 4 + i, e * 4 + (i + (d if e % C == 0 else -d)) % 4) for e in range(Z * Y * C) for i in range(4)
    ]


def cost(flops, nbytes):
    return pl.CostEstimate(flops=flops, bytes_accessed=nbytes, transcendentals=0)


def near(x):
    return pltpu.with_memory_space_constraint(x, pltpu.VMEM)


def near_out(shape, dtype=BF16):
    return pltpu.VMEM(shape, dtype)


def iota(shape, dim):
    return lax.broadcasted_iota(jnp.int32, shape, dim)


def dot(a, b):
    return jnp.dot(a, b, preferred_element_type=F32)


def swap_matrix():
    out_row, in_row = iota((256, 256), 0), iota((256, 256), 1)
    return jnp.where((out_row // SUB == in_row % SUB) & (out_row % SUB == in_row // SUB), 1.0, 0.0).astype(BF16)


def stack_blocks(rows):
    return jnp.concatenate([rows[:, k * 128 : (k + 1) * 128] for k in range(SUB)], axis=0)


def tile_rows(rows, groups, scratch, out_hbm, sem):
    wide = jnp.concatenate([stack_blocks(rows[i * 16 : (i + 1) * 16]) for i in range(len(groups))], axis=1)
    tiled = dot(swap_matrix(), wide).astype(BF16)
    for i, g in enumerate(groups):
        scratch[g * 256 : (g + 1) * 256, :] = tiled[:, i * 128 : (i + 1) * 128]
    here = pl.ds(groups[0] * 256, len(groups) * 256)
    copy = pltpu.make_async_copy(scratch.at[here, :], out_hbm.at[here, :], sem)
    copy.start()
    return copy


def untile_groups(in_ref, groups, place):
    wide = jnp.concatenate([in_ref[g * 256 : (g + 1) * 256, :] for g in groups], axis=1)
    y = dot(swap_matrix(), wide).astype(BF16)
    for i, g in enumerate(groups):
        ref, row = place(g)
        for k in range(SUB):
            ref[row : row + 16, k * 128 : (k + 1) * 128] = y[k * SUB : (k + 1) * SUB, i * 128 : (i + 1) * 128]


TILES = [pltpu.VMEM((SLOTS * SUB, 128), BF16), pltpu.SemaphoreType.DMA((3,))]


def own_lanes(ref, tp):
    whole = ref[...].astype(F32)
    return sum(jnp.where(tp == j, whole[:, j * TOK : (j + 1) * TOK], 0.0) for j in range(4))


def column(row):
    n = row.shape[1]
    wide = jnp.broadcast_to(row, (n, n))
    return jnp.sum(jnp.where(iota((n, n), 0) == iota((n, n), 1), wide, 0.0), axis=1, keepdims=True)


def pair_slots(route_ref, tp):
    routes = own_lanes(route_ref, tp)
    row = jnp.concatenate([routes[0:1], routes[1:2]], axis=1)
    wide = jnp.broadcast_to(row, (128, 128))
    same = jnp.broadcast_to(column(row), (128, 128)) == wide
    earlier = iota((128, 128), 0) % TOK < iota((128, 128), 1) % TOK
    rank = jnp.sum(jnp.where(same & earlier, 1.0, 0.0), axis=0, keepdims=True)
    return row * CAP + rank


def prep_kernel(tp_ref, x_hbm, gain_hbm, route_hbm, out_hbm, x_ref, gain_ref, route_ref, loaded, scratch, sems):
    tp = tp_ref[0]
    mine = x_hbm.at[pl.ds(pl.multiple_of(tp * TOK, TOK), TOK), :]
    pairs = ((route_hbm, route_ref), (mine, x_ref), (gain_hbm, gain_ref))
    copies = [pltpu.make_async_copy(here, there, loaded.at[i]) for i, (here, there) in enumerate(pairs)]
    for copy in copies:
        copy.start()
    copies[0].wait()
    slots = jnp.broadcast_to(pair_slots(route_ref, tp), (SLOTS, 128))
    chosen = jnp.where(iota((SLOTS, 128), 0).astype(F32) == slots, 1.0, 0.0)
    select = (chosen[:, :TOK] + chosen[:, TOK:]).astype(BF16)
    copies[1].wait()
    copies[2].wait()
    x = x_ref[...].astype(F32)
    scale = lax.rsqrt(jnp.mean(x * x, axis=-1, keepdims=True) + 1e-06)
    normed = (x * scale * gain_ref[...].astype(F32).reshape(1, D)).astype(BF16)
    sent = dot(select, normed).astype(BF16)
    copies = [
        tile_rows(sent[part * 64 : (part + 1) * 64], range(part * 4, part * 4 + 4), scratch, out_hbm, sems.at[part])
        for part in range(3)
    ]
    for copy in copies:
        copy.wait()


def prep(tp, routed_input, gain, routes):
    return pl.pallas_call(
        prep_kernel,
        in_specs=[SMEM, HBM, HBM, HBM],
        out_specs=HBM,
        out_shape=pltpu.HBM((SLOTS * SUB, 128), BF16),
        scratch_shapes=[
            pltpu.VMEM((TOK, D), BF16),
            pltpu.VMEM((D,), BF16),
            pltpu.VMEM((2, 4 * TOK), jnp.int32),
            pltpu.SemaphoreType.DMA((3,)),
        ]
        + TILES,
        cost_estimate=cost(400_000_000, 2_000_000),
        name="prep",
        compiler_params=LIMIT,
    )(tp, *(pltpu.with_memory_space_constraint(x, pltpu.HBM) for x in (routed_input, gain, routes.T)))


def untile_kernel(a_hbm, top_ref, bottom_ref, scratch, sems):
    copies = []
    for part in range(3):
        here = pl.ds(part * 1024, 1024)
        copies.append(pltpu.make_async_copy(a_hbm.at[here, :], scratch.at[here, :], sems.at[part]))
        copies[-1].start()
    for part in range(3):
        copies[part].wait()
        untile_groups(
            scratch,
            range(part * 4, part * 4 + 4),
            lambda g: (top_ref, g * 16) if g < TOP // 16 else (bottom_ref, g * 16 - TOP),
        )


def untile(a):
    return pl.pallas_call(
        untile_kernel,
        out_shape=[near_out((TOP, D)), near_out((SLOTS - TOP, D))],
        in_specs=[HBM],
        out_specs=[VMEM] * 2,
        scratch_shapes=TILES,
        cost_estimate=cost(400_000_000, 1_600_000),
        name="untile",
        compiler_params=LIMIT,
    )(pltpu.with_memory_space_constraint(a, pltpu.HBM))


def rows_kernel(count, *refs):
    blocks, (gate_ref, up_ref, down_ref), outs = refs[: -count - 3], refs[-count - 3 : -count], refs[-count:]
    x = jnp.concatenate([ref[...] for ref in blocks], axis=0)
    gate = dot(x, gate_ref[0])
    upper = dot(x, up_ref[0])
    hidden = (gate / (1.0 + jnp.exp(-gate)) * upper).astype(BF16)
    result = dot(hidden, down_ref[0]).astype(BF16)
    at = 0
    for out in outs:
        out[...] = result[at : at + out.shape[0]]
        at += out.shape[0]


def expert_rows(weights, pieces, *blocks):
    rows = sum(b.shape[0] for b in blocks)
    return pl.pallas_call(
        functools.partial(rows_kernel, len(pieces)),
        out_shape=[place((count, D), BF16) for count, place in pieces],
        in_specs=[VMEM] * (len(blocks) + 3),
        out_specs=[VMEM] * len(pieces),
        cost_estimate=cost(3_000_000 * rows, 8_000 * rows),
        name="expert_rows",
        compiler_params=LIMIT,
    )(*(near(b) for b in blocks), *weights)


def add_kernel(a_ref, b_ref, c_ref, d_ref, ab_ref, cd_ref):
    ab_ref[...] = (a_ref[...].astype(F32) + b_ref[...].astype(F32)).astype(BF16)
    cd_ref[...] = (c_ref[...].astype(F32) + d_ref[...].astype(F32)).astype(BF16)


def add_pairs(kept_a, came_a, kept_b, came_b):
    return pl.pallas_call(
        add_kernel,
        out_shape=[near_out((QUARTER, D))] * 2,
        in_specs=[VMEM] * 4,
        out_specs=[VMEM] * 2,
        cost_estimate=cost(10_000_000, 1_200_000),
        name="add_pairs",
        compiler_params=LIMIT,
    )(kept_a, near(came_a), kept_b, near(came_b))


def total1_kernel(own_ref, *refs):
    early, late, (out_hbm, sum_ref, scratch, sems) = refs[:4], refs[4:6], refs[6:]
    copies = []
    for half in range(2):
        first = slice(half * TOP, half * TOP + QUARTER)
        second = slice(half * TOP + QUARTER, (half + 1) * TOP)
        added = own_ref[first, :].astype(F32) + (early[half * 2][...].astype(F32) + late[half][...].astype(F32))
        copies.append(tile_rows(added.astype(BF16), range(half * 6, half * 6 + 3), scratch, out_hbm, sems.at[half]))
        sum_ref[half] = own_ref[second, :].astype(F32) + early[half * 2 + 1][...].astype(F32)
    for copy in copies:
        copy.wait()


def total1(*parts):
    return pl.pallas_call(
        total1_kernel,
        out_shape=[pltpu.HBM((SLOTS * SUB, 128), BF16), near_out((2, QUARTER, D), F32)],
        in_specs=[VMEM] * 7,
        out_specs=[HBM, VMEM],
        scratch_shapes=TILES,
        cost_estimate=cost(200_000_000, 3_000_000),
        name="total1",
        compiler_params=LIMIT,
    )(*(near(p) for p in parts))


def total2_kernel(begun_hbm, sum_ref, top2_ref, bottom2_ref, out_hbm, scratch, sems):
    copies = []
    for half, late in enumerate((top2_ref, bottom2_ref)):
        added = sum_ref[half] + late[...].astype(F32)
        groups = range(half * 6 + 3, half * 6 + 6)
        copies.append(tile_rows(added.astype(BF16), groups, scratch, out_hbm, sems.at[half]))
    for copy in copies:
        copy.wait()


def total2(begun, *parts):
    return pl.pallas_call(
        total2_kernel,
        out_shape=pltpu.HBM((SLOTS * SUB, 128), BF16),
        in_specs=[HBM] + [VMEM] * 3,
        out_specs=HBM,
        scratch_shapes=TILES,
        input_output_aliases={0: 0},
        cost_estimate=cost(200_000_000, 1_500_000),
        name="total2",
        compiler_params=LIMIT,
    )(begun, *(near(p) for p in parts))


def choose_kernel(tp_ref, route_ref, weight_ref, pick_ref, scale_ref):
    tp = tp_ref[0]
    slots = pair_slots(route_ref, tp)
    weights = own_lanes(weight_ref, tp)
    for k in range(2):
        rows = slice(k * TOK, (k + 1) * TOK)
        slot = jnp.broadcast_to(column(slots[:, rows]), (TOK, SLOTS))
        pick_ref[rows, :] = jnp.where(iota((TOK, SLOTS), 1).astype(F32) == slot, 1.0, 0.0).astype(BF16)
        scale_ref[rows, :] = column(weights[k : k + 1])


def choose(tp, routes, route_weight):
    return pl.pallas_call(
        choose_kernel,
        in_specs=[SMEM] + [VMEM] * 2,
        out_specs=[VMEM] * 2,
        out_shape=[near_out((2 * TOK, SLOTS)), near_out((2 * TOK, 1), F32)],
        cost_estimate=cost(10_000_000, 100_000),
        name="choose",
        compiler_params=LIMIT,
    )(tp, routes.T, route_weight.T)


def combine_kernel(r_ref, pick_ref, scale_ref, o_ref, plain):
    for part in range(3):
        untile_groups(r_ref, range(part * 4, part * 4 + 4), lambda g: (plain, g * 16))
    picked = dot(pick_ref[...], plain[...]) * scale_ref[...]
    o_ref[...] = (picked[:TOK] + picked[TOK:]).astype(BF16)


def combine(back, picks, scales):
    return pl.pallas_call(
        combine_kernel,
        in_specs=[VMEM] * 3,
        out_specs=VMEM,
        out_shape=jax.ShapeDtypeStruct((TOK, D), BF16),
        scratch_shapes=[pltpu.VMEM((SLOTS, D), BF16)],
        cost_estimate=cost(400_000_000, 2_000_000),
        name="combine",
        compiler_params=LIMIT,
    )(near(back), near(picks), near(scales))


def attend_kernel(last, ep_ref, tp_ref, q_hbm, gate_hbm, blocks_ref, *refs):
    q_ref, gate_ref, sems = refs[-3:]
    refs = refs[:-3]
    carried, refs = (refs[:3], refs[3:]) if last else ((), refs)
    outs, (best, total, summed, out_ref) = (refs[:4], refs[4:]) if last else ((), refs + (None,))
    copies = [
        pltpu.make_async_copy(here, there, sems.at[i])
        for i, (here, there) in enumerate(((q_hbm, q_ref), (gate_hbm, gate_ref)))
    ]
    for copy in copies:
        copy.start()
    for copy in copies:
        copy.wait()
    me = ep_ref[0]
    plane, row, core = me // 8, (me // 2) % 4, me % 2
    core = 1 - core if last else core
    q = q_ref[...].astype(F32) * 0.125
    q = jnp.concatenate([q[:, :64], q[:, 64:]], axis=0).astype(BF16)
    col = column(gate_ref[:, pl.ds(pl.multiple_of(me * 128, 128), 128)])
    gate_col = jnp.concatenate([col, col], axis=0)

    def blocks_of(planes, low, high):
        return jnp.concatenate([blocks_ref[z * 4 + i, low:high, :] for z in planes for i in range(4)], axis=1)

    def starts_of(planes):
        return [((z * 4 + (row + dy + 4) % 4) * 2 + core) * 128 for z in planes for dy in ROW_OFFSETS]

    def scores_of(planes):
        gates = [gate_ref[:, pl.ds(pl.multiple_of(at, 128), 128)] for at in starts_of(planes)]
        return dot(q, blocks_of(planes, 0, 64)) + gate_col - jnp.concatenate(gates, axis=1)

    def weighted(weights, planes):
        return lax.dot_general(
            weights.astype(BF16),
            blocks_of(planes, 64, 128),
            (((1,), (1,)), ((), ())),
            preferred_element_type=F32,
        )

    def merge(scores, planes, before, count, product):
        top = jnp.maximum(before, jnp.max(scores, axis=1, keepdims=True))
        factor = jnp.exp(before - top)
        weights = jnp.exp(scores - top)
        best[...] = top
        total[...] = count * factor + jnp.sum(weights, axis=1, keepdims=True)
        summed[...] = product * factor + weighted(weights, planes)

    scores = scores_of((plane,))
    query = iota((256, 128), 0) % 128 + me * 128
    allowed = jnp.concatenate([iota((256, 128), 1) + at <= query for at in starts_of((plane,))], axis=1)
    scores = jnp.where(allowed, scores, -jnp.inf)
    if last:
        merge(scores, (plane,), *(ref[...] for ref in carried))
    else:
        top = jnp.max(scores, axis=1, keepdims=True)
        weights = jnp.exp(scores - top)
        best[...] = top
        total[...] = jnp.sum(weights, axis=1, keepdims=True)
        summed[...] = weighted(weights, (plane,))

    @pl.loop(0, plane // 2)
    def _(pair):
        planes = (pair * 2, pair * 2 + 1)
        merge(scores_of(planes), planes, best[...], total[...], summed[...])

    @pl.when(plane % 2 == 1)
    def _():
        planes = (plane - 1,)
        merge(scores_of(planes), planes, best[...], total[...], summed[...])

    if last:
        out = summed[...] / total[...]
        out_ref[...] = jnp.concatenate([out[:128], out[128:]], axis=1)
        for ref, shift in zip(outs, TP_SHIFTS):
            at = pl.multiple_of((tp_ref[0] + shift + 4) % 4 * 32, 32)
            ref[...] = out_ref[pl.ds(at, 32), :].astype(BF16)


STATE = ((256, 1), (256, 1), (256, 64))
LOADED = [pltpu.VMEM((128, 128), BF16), pltpu.VMEM((1, 8192), F32), pltpu.SemaphoreType.DMA((2,))]


def far_off(*arrays):
    return tuple(pltpu.with_memory_space_constraint(x, pltpu.HBM) for x in arrays)


def attend_same(ep, tp, queries, cum_gate, blocks):
    return pl.pallas_call(
        functools.partial(attend_kernel, False),
        out_shape=[near_out(shape, F32) for shape in STATE],
        in_specs=[SMEM] * 2 + [HBM] * 2 + [VMEM],
        out_specs=[VMEM] * 3,
        scratch_shapes=LOADED,
        cost_estimate=cost(2_000_000_000, 1_500_000),
        name="attend_same",
        compiler_params=LIMIT,
    )(ep, tp, *far_off(queries, cum_gate), near(blocks))


def attend_other(ep, tp, queries, cum_gate, blocks, state):
    return pl.pallas_call(
        functools.partial(attend_kernel, True),
        out_shape=[near_out((32, 128))] * 4,
        in_specs=[SMEM] * 2 + [HBM] * 2 + [VMEM] * 4,
        out_specs=[VMEM] * 4,
        scratch_shapes=[pltpu.VMEM(shape, F32) for shape in STATE + ((128, 128),)] + LOADED,
        cost_estimate=cost(2_000_000_000, 1_500_000),
        name="attend_other",
        compiler_params=LIMIT,
    )(ep, tp, *far_off(queries, cum_gate), near(blocks), *(near(x) for x in state))


def project_kernel(tp_ref, a_ref, b_ref, c_ref, d_ref, w_ref, o_ref):
    added = None
    for ref, shift in zip((a_ref, b_ref, c_ref, d_ref), TP_SHIFTS):
        at = pl.multiple_of((tp_ref[0] - shift + 4) % 4 * 128, 128)
        term = dot(ref[...], w_ref[pl.ds(at, 128), :])
        added = term if added is None else added + term
    o_ref[...] = added.astype(BF16)


def project(tp, parts, out_weight):
    return pl.pallas_call(
        project_kernel,
        out_shape=jax.ShapeDtypeStruct((32, D), BF16),
        in_specs=[SMEM] + [VMEM] * 5,
        out_specs=VMEM,
        cost_estimate=cost(70_000_000, 2_300_000),
        name="project",
        compiler_params=LIMIT,
    )(tp, *(near(p) for p in parts), out_weight)


def over_experts(x):
    return lax.all_to_all(x.reshape(EXPERTS, 48, 128), "ep", 0, 0, tiled=True).reshape(SLOTS * SUB, 128)


def repeat_kernel(a_ref, b_ref, c_ref, d_ref, o_ref):
    for i, ref in enumerate((a_ref, b_ref, c_ref, d_ref)):
        for z in range(Z):
            o_ref[z, i] = ref[...]


def repeated(*blocks):
    return pl.pallas_call(
        repeat_kernel,
        out_shape=pltpu.HBM((Z, 4, 128, 128), BF16),
        in_specs=[VMEM] * 4,
        out_specs=VMEM,
        cost_estimate=cost(1_000_000, 1_200_000),
        name="repeat",
        compiler_params=LIMIT,
    )(*(near(b) for b in blocks))


def over_planes(own):
    return lax.all_to_all(own, "ep", 0, 0, tiled=True, axis_index_groups=PLANES).reshape(32, 128, 128)


def gather_kv(key_cache, value_cache):
    kv = jnp.concatenate([key_cache[0], value_cache[0]], axis=0)
    ring = repeated(
        kv, lax.ppermute(kv, "ep", y_perm(1)), lax.ppermute(kv, "ep", y_perm(-1)), lax.ppermute(kv, "ep", y_perm(2))
    )
    same = over_planes(ring)
    return same, lax.ppermute(same, "ep", core_perm())


def body(
    queries,
    key_cache,
    value_cache,
    cum_gate,
    out_weight,
    routed_input,
    norm_gain,
    routes,
    route_weight,
    expert_gate,
    expert_up,
    expert_down,
):
    tp = lax.axis_index("tp").astype(jnp.int32).reshape(1)
    ep = lax.axis_index("ep").astype(jnp.int32).reshape(1)
    weights = (near(expert_gate), near(expert_up), near(expert_down))
    came = over_experts(prep(tp, routed_input, norm_gain, routes))
    own_top, own_bottom = untile(came)
    left_top = lax.ppermute(own_top, ("ep", "tp"), ring_perm(1))
    right_bottom = lax.ppermute(own_bottom, ("ep", "tp"), ring_perm(-1))
    left_bottom = lax.ppermute(own_bottom, ("ep", "tp"), ring_perm(1))
    right_top = lax.ppermute(own_top, ("ep", "tp"), ring_perm(-1))
    far_top = lax.ppermute(left_top, ("ep", "tp"), ring_perm(1))
    far_bottom = lax.ppermute(right_bottom, ("ep", "tp"), ring_perm(-1))
    kept, sent = (QUARTER, pltpu.HBM), (QUARTER, pltpu.VMEM)
    (own_part,) = expert_rows(weights, ((SLOTS, pltpu.VMEM),), own_top, own_bottom)
    early1, early2, left1, left2, right1, right2, early3, early4 = expert_rows(
        weights, (sent, sent, kept, kept, kept, kept, sent, sent), left_top, left_bottom, right_top, right_bottom
    )
    top1, top2, bottom1, bottom2 = expert_rows(weights, ((QUARTER, pltpu.VMEM),) * 4, far_top, far_bottom)
    early = (
        lax.ppermute(early1, ("ep", "tp"), ring_perm(-1)),
        lax.ppermute(early2, ("ep", "tp"), ring_perm(-1)),
        lax.ppermute(early3, ("ep", "tp"), ring_perm(1)),
        lax.ppermute(early4, ("ep", "tp"), ring_perm(1)),
    )
    late = []
    for top, bottom, left, right in ((top1, bottom1, left1, right1), (top2, bottom2, left2, right2)):
        passed_top = lax.ppermute(top, ("ep", "tp"), ring_perm(1))
        passed_bottom = lax.ppermute(bottom, ("ep", "tp"), ring_perm(-1))
        right, left = add_pairs(right, passed_top, left, passed_bottom)
        late.append((lax.ppermute(right, ("ep", "tp"), ring_perm(1)), lax.ppermute(left, ("ep", "tp"), ring_perm(-1))))
    (late_top1, late_bottom1), (late_top2, late_bottom2) = late
    mine, sums = total1(own_part, *early, late_top1, late_bottom1)
    mine = total2(mine, sums, late_top2, late_bottom2)
    picks, scales = choose(tp, routes, route_weight)
    expert_out = combine(over_experts(mine), picks, scales)

    same, other = gather_kv(key_cache, value_cache)
    state = attend_same(ep, tp, queries, cum_gate, same)
    rows, up, down, across = attend_other(ep, tp, queries, cum_gate, other, state)
    parts = (
        rows,
        lax.ppermute(up, "tp", tp_perm(1)),
        lax.ppermute(down, "tp", tp_perm(-1)),
        lax.ppermute(across, "tp", tp_perm(2)),
    )
    mixed_out = project(tp, parts, out_weight)
    return (mixed_out, expert_out)


def solution(mesh):
    return jax.shard_map(
        body,
        mesh=mesh,
        in_specs=(
            P("ep", "tp"),
            P("tp", None, "ep"),
            P("tp", None, "ep"),
            P("tp", None),
            P(),
            P("ep", None),
            P(),
            P("ep", None),
            P("ep", None),
            P("ep", None, "tp"),
            P("ep", None, "tp"),
            P("ep", "tp", None),
        ),
        out_specs=(P(("ep", "tp"), None), P(("ep", "tp"), None)),
        check_vma=False,
    )
```
